1024 devices in a mesh: sp: 128 (over z, y), tp: 8 (over x, core).
Axes of the slice: x: 4, y: 4, z: 32, core: 2. Of those that a mesh axis runs over, the one named last changes fastest.
Arguments:
- tokens: bfloat16 [49152, 2048], P('sp'), may hold values from -6 to 6
- norm_gain: float32 [2048], replicated, may hold values from 0.1 to 12
- w_query: bfloat16 [3, 512, 2048], P(None, 'tp'), may hold values from -0.125 to 0.125
- w_key: bfloat16 [3, 512, 2048], P(None, 'tp'), may hold values from -0.125 to 0.125
- w_value: bfloat16 [3, 512, 2048], P(None, 'tp'), may hold values from -0.125 to 0.125
- w_out: bfloat16 [512, 2048], P(None, 'tp'), may hold values from -0.25 to 0.25
Outputs:
- projected: bfloat16 [49152, 2048], P('sp', 'tp')
- log_weight: float32 [8, 49152], P('tp', 'sp')
The draws below stay inside these ranges and needn't reach their ends.
All inputs are finite; a program needn't handle non-finite values.
Results may differ from the reference program's by a relative error of at most 0.006.
The reference program's roundings to bfloat16 on the way count: a program that leaves them out, or rounds other values in their place, can miss the bound.
Values may be sent and summed in bfloat16 or wider, within the bound.
No kernel may reach another device: no remote copies, remote signals or barrier semaphores. Data moves between devices by JAX's collectives and lax.ppermute only.
A program may use at most 32 MiB of HBM per device.

```python
import math
import jax
import jax.numpy as jnp
from jax import lax

D = 2048
HEAD_DIM = 64
SLOTS = 8
STEPS = 128
MIDDLE_DILATION = 4
WIDE_DILATION = 16
TOK_DEV = 384
TOKENS = 49152


def draw_norm_gain(key, part):
    return 1.0 + 0.18 * jnp.clip(jax.random.normal(key, (D,), jnp.float32), -5.0, 5.0)


def levels(own_key, dims, split, least, largest):
    factor_of, own = 1.0, jax.random.fold_in(own_key, 6)
    for position, parts in split:
        steps = jnp.exp(jax.random.uniform(jax.random.fold_in(own, position), (parts,), jnp.float32, least / len(split), largest / len(split)))
        factor_of = factor_of * jnp.repeat(steps, dims[position] // parts).reshape([-1 if axis == position else 1 for axis in range(len(dims))])
    return factor_of


def gaussian(stream_key, dims, deviation, reach, shards=(), kind=jnp.bfloat16):
    loudness = levels(stream_key, dims, shards, -0.22, 0.18) if shards else 1.0
    array = jax.random.normal(stream_key, dims, jnp.float32) * deviation * loudness
    return jnp.minimum(jnp.maximum(array, -reach), reach).astype(kind)


def setup_inputs(seed: int = 0) -> dict:
    key_list = jax.random.split(jax.random.key(seed), 7)
    tokens = gaussian(key_list[0], (TOKENS, D), 1.0, 6.0, ((0, 128),))
    norm_gain = draw_norm_gain(jax.random.fold_in(key_list[6], 71), 0)
    w_query = gaussian(key_list[2], (3, SLOTS * HEAD_DIM, D), D ** -0.5, 0.125, ((1, 8),))
    w_key = gaussian(key_list[3], (3, SLOTS * HEAD_DIM, D), D ** -0.5, 0.125, ((1, 8),))
    w_value = gaussian(key_list[4], (3, SLOTS * HEAD_DIM, D), D ** -0.5, 0.125, ((1, 8),))
    w_out = gaussian(key_list[5], (SLOTS * HEAD_DIM, D), (SLOTS * HEAD_DIM) ** -0.5, 0.25, ((1, 8),))
    return {"tokens": tokens, "norm_gain": norm_gain, "w_query": w_query, "w_key": w_key, "w_value": w_value, "w_out": w_out}


NEG_BIG = -1e+30

def attend(query, context, first_pos, dilation_step, slopes):
    head_count = slopes.shape[0]
    width = query.shape[1] // head_count
    row_count = query.shape[0]
    query_len = row_count // dilation_step
    key_len = context.shape[0] // dilation_step
    query_heads = query.reshape(query_len, dilation_step, head_count, width).transpose(1, 2, 0, 3)
    split_context = context.reshape(key_len, dilation_step, 2, head_count, width)
    key_heads = split_context[:, :, 0].transpose(1, 2, 0, 3)
    value_heads = split_context[:, :, 1].transpose(1, 2, 0, 3)
    scores = jnp.einsum('rhqe,rhke->rhqk', query_heads.astype(jnp.float32), key_heads.astype(jnp.float32)) * (1.0 / math.sqrt(width))
    query_index = jnp.arange(query_len, dtype=jnp.int32)[:, None]
    key_index = jnp.arange(key_len, dtype=jnp.int32)[None, :]
    distance = query_index + STEPS - key_index
    residue = jnp.arange(dilation_step, dtype=jnp.int32)[:, None, None, None]
    key_pos = first_pos - STEPS * dilation_step + key_index[None, None] * dilation_step + residue
    valid = (distance >= 0) & (distance <= STEPS) & (key_pos >= 0)
    logits = scores - slopes[None, :, None, None] * distance.astype(jnp.float32)
    logits = jnp.where(valid, logits, NEG_BIG)
    row_max = lax.optimization_barrier(jnp.max(logits, axis=-1, keepdims=True))
    row_sum = lax.optimization_barrier(jnp.sum(jnp.exp(logits - row_max), axis=-1, keepdims=True))
    log_total = row_max + jnp.log(row_sum)
    weights = jnp.exp(logits - log_total).astype(jnp.bfloat16)
    outputs = jnp.einsum('rhqk,rhke->rhqe', weights.astype(jnp.float32), value_heads.astype(jnp.float32))
    outputs = outputs.transpose(2, 0, 1, 3).reshape(row_count, head_count, width)
    log_total = log_total[..., 0].transpose(2, 0, 1).reshape(row_count, head_count)
    return (outputs, log_total)

def reference(tokens, norm_gain, w_query, w_key, w_value, w_out):
    total_rows = tokens.shape[0]
    scaled = tokens.astype(jnp.float32)
    normed = (scaled * lax.rsqrt(lax.optimization_barrier(jnp.mean(scaled * scaled, axis=-1, keepdims=True)) + 1e-06) * norm_gain).astype(jnp.bfloat16)
    normed_wide = normed.astype(jnp.float32)
    query_rows = jnp.einsum('td,gcd->gtc', normed_wide, w_query.astype(jnp.float32)).astype(jnp.bfloat16)
    keys = jnp.einsum('td,gcd->gtc', normed_wide, w_key.astype(jnp.float32)).astype(jnp.bfloat16)
    value_rows = jnp.einsum('td,gcd->gtc', normed_wide, w_value.astype(jnp.float32)).astype(jnp.bfloat16)
    slot_ids = jnp.arange(SLOTS, dtype=jnp.int32)
    blocks = total_rows // TOK_DEV
    dilation_list = (1, MIDDLE_DILATION, WIDE_DILATION)
    outputs_all = []
    logs_all = []
    for cohort in range(3):
        dilation_step = dilation_list[cohort]
        slopes = jnp.exp2(-8.0 * (cohort * SLOTS + slot_ids + 1).astype(jnp.float32) / (3 * SLOTS))
        key_value = jnp.concatenate([keys[cohort], value_rows[cohort]], axis=-1)
        padded = jnp.concatenate([jnp.zeros((STEPS * dilation_step, key_value.shape[1]), jnp.bfloat16), key_value], axis=0)
        query_all = query_rows[cohort]

        def one_block(block_number):
            start = block_number * TOK_DEV
            query_block = lax.dynamic_slice_in_dim(query_all, start, TOK_DEV, 0)
            context = lax.dynamic_slice_in_dim(padded, start, STEPS * dilation_step + TOK_DEV, 0)
            return attend(query_block, context, start, dilation_step, slopes)
        block_out, block_log = lax.map(one_block, jnp.arange(blocks, dtype=jnp.int32))
        outputs_all.append(block_out.reshape(total_rows, SLOTS, HEAD_DIM))
        logs_all.append(block_log.reshape(total_rows, SLOTS))
    stacked = jnp.stack(logs_all)
    log_weight = jax.nn.logsumexp(stacked, axis=0)
    shares = jnp.exp(stacked - log_weight[None])
    mixture = lax.optimization_barrier(jnp.sum(shares[..., None] * jnp.stack(outputs_all), axis=0))
    mixture = mixture.reshape(total_rows, SLOTS * HEAD_DIM).astype(jnp.bfloat16)
    projected = jnp.dot(mixture, w_out, preferred_element_type=jnp.float32).astype(jnp.bfloat16)
    return (projected, log_weight.T)
```

```python
import jax
import jax.numpy as jnp
from jax import lax
from jax.experimental import pallas as pl
from jax.experimental.pallas import tpu as pltpu
from jax.sharding import PartitionSpec as P

HEAD_DIM = 64
SLOTS = 8
STEPS = 128
GROUPS = 3
MIDDLE_DILATION = 4
WIDE_DILATION = 16
NEG_BIG = -1e30

CLASSES = 4
NT = (((1,), (1,)), ((), ()))
NN = (((1,), (0,)), ((), ()))
TN = (((0,), (0,)), ((), ()))


def dot(a, b, dims):
    return lax.dot_general(a, b, dims, preferred_element_type=jnp.float32)


def iota(shape, dim):
    return lax.broadcasted_iota(jnp.int32, shape, dim)


def position_of_row(p, rows):
    per_class = rows // CLASSES
    per_residue = rows // WIDE_DILATION
    c = p // per_class
    rest = p - c * per_class
    j = rest // per_residue
    i = rest - j * per_residue
    return c, j, i


def project_kernel(tokens_ref, gain_ref, wq_ref, wk_ref, wv_ref, q_ref, kv0_ref, s1_ref, s2_ref, s3_ref, w_ref):
    rows, _ = tokens_ref.shape
    x = tokens_ref[...].astype(jnp.float32)
    mean = jnp.mean(x * x, axis=-1, keepdims=True)
    normed = (x * lax.rsqrt(mean + 1e-6) * gain_ref[...]).astype(jnp.bfloat16)
    for g in range(GROUPS):
        w_ref[g * 128 : g * 128 + 64, :] = wk_ref[g]
        w_ref[g * 128 + 64 : g * 128 + 128, :] = wv_ref[g]
    kv = dot(normed, w_ref[...], NT).astype(jnp.bfloat16)
    c, j, i = position_of_row(iota((rows, rows), 0), rows)
    pick = (16 * i + 4 * j + c == iota((rows, rows), 1)).astype(jnp.bfloat16)
    kv = dot(pick, kv, NN).astype(jnp.bfloat16)
    halo = STEPS // WIDE_DILATION
    per_residue = rows // WIDE_DILATION
    for g, ref, at in ((0, s1_ref, 0), (1, s2_ref, 0)):
        for r in range(WIDE_DILATION):
            lo = r * per_residue + per_residue - halo
            ref[at + r * halo : at + (r + 1) * halo, :] = kv[lo : lo + halo, g * 128 : (g + 1) * 128]
    kv0_ref[...] = kv[:, 0:128]
    s1_ref[STEPS : STEPS + rows, :] = kv[:, 128:256]
    s1_ref[STEPS + rows : STEPS + 2 * rows, :] = kv[:, 256:384]
    s2_ref[STEPS : STEPS + rows, :] = kv[:, 256:384]
    s3_ref[...] = kv[:, 256:384]
    wq = wq_ref[...].reshape(GROUPS * HEAD_DIM, -1)
    q = (dot(normed, wq, NT).astype(jnp.bfloat16) * jnp.bfloat16(0.125)).astype(jnp.bfloat16)
    q_ref[...] = dot(pick, q, NN).astype(jnp.bfloat16)


def softmax_pieces(scores):
    top = jnp.max(scores, axis=-1, keepdims=True)
    e = jnp.exp(scores - top)
    total = jnp.sum(e, axis=-1, keepdims=True)
    return (e / total).astype(jnp.bfloat16), top + jnp.log(total)


def bias_of(distance, valid, slope):
    ok = valid & (distance >= 0) & (distance <= STEPS)
    return jnp.where(ok, -slope * distance.astype(jnp.float32), NEG_BIG)


def key_rows(rows, keys, has_halo):
    del has_halo
    per_class = rows // CLASSES
    per_residue = rows // WIDE_DILATION
    halo = STEPS // WIDE_DILATION
    n = iota((per_class, keys), 1)
    full = keys // per_class
    b = n // per_class
    rest = n - b * per_class
    j = rest // per_residue
    i = rest - j * per_residue
    tail = n - full * per_class
    jt = tail // halo
    it = tail - jt * halo + per_residue - halo
    at_tail = b >= full
    return jnp.where(at_tail, jt, j), jnp.where(at_tail, it, i), b


def near_kernel(sp_ref, slope_ref, q_ref, kv0_ref, s1_ref, r1_ref, r2_ref, o0_ref, l0_ref, o1_ref, l1_ref):
    rows = kv0_ref.shape[0]
    sp = sp_ref[0]
    per_class = rows // CLASSES
    per_residue = rows // WIDE_DILATION
    halo = STEPS // WIDE_DILATION
    c, j, i = position_of_row(iota((rows, rows + STEPS), 0), rows)
    tq = 16 * i + 4 * j + c
    n = iota((rows, rows + STEPS), 1)
    c, j, i = position_of_row(n, rows)
    tail = n - rows
    r = tail // halo
    it = tail - r * halo + per_residue - halo
    t_tail = 16 * it + 4 * (r % 4) + r // 4 - rows
    is_tail = n >= rows
    tk = jnp.where(is_tail, t_tail, 16 * i + 4 * j + c)
    bias = bias_of(tq - tk, jnp.logical_or(jnp.logical_not(is_tail), sp >= 1), slope_ref[0])
    keys = jnp.concatenate([kv0_ref[...], r1_ref[0:STEPS, :]], axis=0)
    scores = dot(q_ref[:, 0:64], keys[:, 0:64], NT) + bias
    p, l = softmax_pieces(scores)
    o0_ref[...] = dot(p, keys[:, 64:128], NN)
    l0_ref[...] = l
    n_keys = 2 * per_class + STEPS // CLASSES
    q_row = iota((per_class, n_keys), 0)
    jq = q_row // per_residue
    iq = q_row - jq * per_residue
    jk, ik, b = key_rows(rows, n_keys, True)
    bias = bias_of(4 * (iq - ik) + jq - jk + per_class * b, b <= sp, slope_ref[1])
    for c in range(CLASSES):
        lo = STEPS + c * per_class
        keys = jnp.concatenate(
            [s1_ref[lo : lo + per_class, :], r1_ref[lo : lo + per_class, :], r2_ref[c * 32 : (c + 1) * 32, :]], axis=0
        )
        q = q_ref[c * per_class : (c + 1) * per_class, 64:128]
        p, l = softmax_pieces(dot(q, keys[:, 0:64], NT) + bias)
        o1_ref[c * per_class : (c + 1) * per_class, :] = dot(p, keys[:, 64:128], NN)
        l1_ref[c * per_class : (c + 1) * per_class, :] = l


def wide_kernel(sp_ref, slope_ref, q_ref, s3_ref, r1_ref, r2_ref, r3_ref, r4_ref, o0_ref, l0_ref, o1_ref, l1_ref, mix_ref, lw_ref, mixed_ref, l_ref):
    rows = s3_ref.shape[0]
    sp = sp_ref[0]
    per_class = rows // CLASSES
    per_residue = rows // WIDE_DILATION
    n_keys = 6 * per_class + STEPS // CLASSES
    q_row = iota((per_class, n_keys), 0)
    jq = q_row // per_residue
    iq = q_row - jq * per_residue
    jk, ik, b = key_rows(rows, n_keys, True)
    bias = bias_of(iq - ik + per_residue * b, (jq == jk) & (b <= sp), slope_ref[2])
    for c in range(CLASSES):
        lo = c * per_class
        run = pl.ds(lo, per_class)
        keys = jnp.concatenate(
            [
                s3_ref[run, :],
                r1_ref[pl.ds(STEPS + rows + lo, per_class), :],
                r2_ref[pl.ds(STEPS + lo, per_class), :],
                r3_ref[run, :],
                r4_ref[run, :],
                r4_ref[pl.ds(rows + lo, per_class), :],
                r4_ref[pl.ds(2 * rows + c * 32, 32), :],
            ],
            axis=0,
        )
        p, l2 = softmax_pieces(dot(q_ref[run, 128:192], keys[:, 0:64], NT) + bias)
        o2 = dot(p, keys[:, 64:128], NN)
        l0 = l0_ref[run, :]
        l1 = l1_ref[run, :]
        top = jnp.maximum(jnp.maximum(l0, l1), l2)
        lw = top + jnp.log(jnp.exp(l0 - top) + jnp.exp(l1 - top) + jnp.exp(l2 - top))
        mixed = (
            jnp.exp(l0 - lw) * o0_ref[run, :] + jnp.exp(l1 - lw) * o1_ref[run, :] + jnp.exp(l2 - lw) * o2
        )
        mixed_ref[run, :] = mixed.astype(jnp.bfloat16)
        l_ref[run, :] = lw
    c, j, i = position_of_row(iota((rows, rows), 0), rows)
    pick = 16 * i + 4 * j + c == iota((rows, rows), 1)
    mix_ref[...] = dot(mixed_ref[...], pick.astype(jnp.bfloat16), TN).astype(jnp.bfloat16)
    lw_ref[...] = jnp.sum(jnp.where(pick, l_ref[...], 0.0), axis=0, keepdims=True)


def in_vmem():
    return pl.BlockSpec(memory_space=pltpu.VMEM)


def in_smem():
    return pl.BlockSpec(memory_space=pltpu.SMEM)


def call(body, operands, outs, name, scalars=0, scratch=()):
    return pl.pallas_call(
        body,
        in_specs=[in_smem()] * scalars + [in_vmem()] * (len(operands) - scalars),
        out_specs=[in_vmem()] * len(outs),
        out_shape=[jax.ShapeDtypeStruct(s, d) for s, d in outs],
        scratch_shapes=list(scratch),
        name=name,
    )(*operands)


def from_behind(value, by):
    devices = lax.axis_size("sp")
    return lax.ppermute(value, "sp", [(i, (i + by) % devices) for i in range(devices)])


def per_device(tokens, norm_gain, w_query, w_key, w_value, w_out):
    rows = tokens.shape[0]
    bf16, f32 = jnp.bfloat16, jnp.float32
    sp = lax.axis_index("sp").reshape(1)
    slot = lax.axis_index("tp")
    slopes = jnp.exp2(-8.0 * (jnp.arange(GROUPS, dtype=jnp.int32) * SLOTS + slot + 1).astype(f32) / (GROUPS * SLOTS))
    q, kv0, s1, s2, s3 = call(
        project_kernel,
        (tokens, norm_gain.reshape(1, -1), w_query, w_key, w_value),
        [
            ((rows, GROUPS * HEAD_DIM), bf16),
            ((rows, 128), bf16),
            ((STEPS + 2 * rows, 128), bf16),
            ((STEPS + rows, 128), bf16),
            ((rows, 128), bf16),
        ],
        "project",
        scratch=[pltpu.VMEM((GROUPS * 128, tokens.shape[1]), bf16)],
    )
    r1 = from_behind(s1, 1)
    r2 = from_behind(s2, 2)
    r3 = from_behind(s3, 3)
    per_residue, halo = rows // WIDE_DILATION, STEPS // WIDE_DILATION
    second = r2[STEPS:].reshape(WIDE_DILATION, per_residue, 128)[:, per_residue - halo :].reshape(STEPS, 128)
    s4 = jnp.concatenate([s3, r1[STEPS + rows :], second], axis=0)
    r4 = from_behind(s4, 4)
    o0, l0, o1, l1 = call(
        near_kernel,
        (sp, slopes, q, kv0, s1, r1, r2),
        [((rows, HEAD_DIM), f32), ((rows, 1), f32), ((rows, HEAD_DIM), f32), ((rows, 1), f32)],
        "near",
        scalars=2,
    )
    mix, log_weight = call(
        wide_kernel,
        (sp, slopes, q, s3, r1, r2, r3, r4, o0, l0, o1, l1),
        [((HEAD_DIM, rows), bf16), ((1, rows), f32)],
        "wide",
        scalars=2,
        scratch=[pltpu.VMEM((rows, HEAD_DIM), bf16), pltpu.VMEM((rows, 1), f32)],
    )
    devices = lax.axis_size("tp")
    everyone = lax.all_to_all(jnp.broadcast_to(mix[None], (devices, *mix.shape)), "tp", 0, 0, tiled=True)
    projected = dot(everyone.reshape(devices * HEAD_DIM, rows), w_out, TN)
    return projected.astype(bf16), log_weight


def solution(mesh):
    in_specs = (P("sp", None), P(), P(None, "tp", None), P(None, "tp", None), P(None, "tp", None), P(None, "tp"))
    out_specs = (P("sp", "tp"), P("tp", "sp"))
    return jax.shard_map(per_device, mesh=mesh, in_specs=in_specs, out_specs=out_specs, check_vma=False)
```

```python
import jax
import jax.numpy as jnp
from jax import lax
from jax.experimental import pallas as pl
from jax.experimental.pallas import tpu as pltpu
from jax.sharding import PartitionSpec as P


HEAD_DIM = 64
SLOTS = 8
STEPS = 128
GROUPS = 3
WIDE_DILATION = 16
NEG_BIG = -1e30

CLASSES = 4
NT = (((1,), (1,)), ((), ()))
NN = (((1,), (0,)), ((), ()))
TN = (((0,), (0,)), ((), ()))


def dot(a, b, dims):
    return lax.dot_general(a, b, dims, preferred_element_type=jnp.float32)


def iota(shape, dim):
    return lax.broadcasted_iota(jnp.int32, shape, dim)


def position_of_row(p, rows):
    per_class = rows // CLASSES
    per_residue = rows // WIDE_DILATION
    c = p // per_class
    rest = p - c * per_class
    j = rest // per_residue
    i = rest - j * per_residue
    return c, j, i


def to_class_order(rows):
    c, j, i = position_of_row(iota((rows, rows), 0), rows)
    return 16 * i + 4 * j + c == iota((rows, rows), 1)


CHUNK = 128


def project_kernel(tokens_hbm, gain_hbm, wk_hbm, wv_hbm, kv0_ref, s1_ref, s2_ref, s3_ref, normed_ref, x_ref, gain_ref, w_ref, sem):
    rows = x_ref.shape[0]
    chunks = rows // CHUNK
    gain_load = pltpu.make_async_copy(gain_hbm, gain_ref, sem.at[chunks + 2 * GROUPS])
    gain_load.start()
    loads = [
        pltpu.make_async_copy(tokens_hbm.at[pl.ds(n * CHUNK, CHUNK)], x_ref.at[pl.ds(n * CHUNK, CHUNK)], sem.at[n])
        for n in range(chunks)
    ]
    for g in range(GROUPS):
        loads.append(pltpu.make_async_copy(wk_hbm.at[g], w_ref.at[pl.ds(g * 128, 64)], sem.at[chunks + 2 * g]))
        loads.append(pltpu.make_async_copy(wv_hbm.at[g], w_ref.at[pl.ds(g * 128 + 64, 64)], sem.at[chunks + 2 * g + 1]))
    for load in loads:
        load.start()
    gain_load.wait()
    gain = gain_ref[...]
    for n in range(chunks):
        loads[n].wait()
        run = pl.ds(n * CHUNK, CHUNK)
        x = x_ref[run, :].astype(jnp.float32)
        mean = jnp.mean(x * x, axis=-1, keepdims=True)
        normed_ref[run, :] = (x * lax.rsqrt(mean + 1e-6) * gain).astype(jnp.bfloat16)
    for load in loads[chunks:]:
        load.wait()
    kv = dot(normed_ref[...], w_ref[...], NT).astype(jnp.bfloat16)
    kv = dot(to_class_order(rows).astype(jnp.bfloat16), kv, NN).astype(jnp.bfloat16)
    halo = STEPS // WIDE_DILATION
    per_residue = rows // WIDE_DILATION
    for g, ref in ((0, s1_ref), (1, s2_ref)):
        for r in range(WIDE_DILATION):
            lo = r * per_residue + per_residue - halo
            ref[r * halo : (r + 1) * halo, :] = kv[lo : lo + halo, g * 128 : (g + 1) * 128]
    kv0_ref[...] = kv[:, 0:128]
    s1_ref[STEPS : STEPS + rows, :] = kv[:, 128:256]
    s1_ref[STEPS + rows : STEPS + 2 * rows, :] = kv[:, 256:384]
    s2_ref[STEPS : STEPS + rows, :] = kv[:, 256:384]
    s3_ref[...] = kv[:, 256:384]


def query_kernel(normed_ref, wq_ref, q_ref):
    rows = normed_ref.shape[0]
    wq = wq_ref[...].reshape(GROUPS * HEAD_DIM, -1)
    q = (dot(normed_ref[...], wq, NT).astype(jnp.bfloat16) * jnp.bfloat16(0.125)).astype(jnp.bfloat16)
    q_ref[...] = dot(to_class_order(rows).astype(jnp.bfloat16), q, NN).astype(jnp.bfloat16)


def relay_kernel(s3_ref, r1_ref, r2_ref, s4_ref):
    rows = s3_ref.shape[0]
    halo = STEPS // WIDE_DILATION
    per_residue = rows // WIDE_DILATION
    s4_ref[0:rows, :] = s3_ref[...]
    s4_ref[rows : 2 * rows, :] = r1_ref[STEPS + rows : STEPS + 2 * rows, :]
    for r in range(WIDE_DILATION):
        lo = STEPS + r * per_residue + per_residue - halo
        s4_ref[2 * rows + r * halo : 2 * rows + (r + 1) * halo, :] = r2_ref[lo : lo + halo, :]


def slope_of(group, slot):
    n = jnp.full((1, 1), group * SLOTS + 1, jnp.int32) + slot
    return jnp.exp2(-8.0 * n.astype(jnp.float32) / (GROUPS * SLOTS))


def softmax_pieces(scores):
    top = jnp.max(scores, axis=-1, keepdims=True)
    e = jnp.exp(scores - top)
    total = jnp.sum(e, axis=-1, keepdims=True)
    return (e / total).astype(jnp.bfloat16), top + jnp.log(total)


def bias_of(distance, valid, slope):
    ok = valid & (distance >= 0) & (distance <= STEPS)
    return jnp.where(ok, -slope * distance.astype(jnp.float32), NEG_BIG)


def key_rows(rows, keys, has_halo):
    del has_halo
    per_class = rows // CLASSES
    per_residue = rows // WIDE_DILATION
    halo = STEPS // WIDE_DILATION
    n = iota((per_class, keys), 1)
    full = keys // per_class
    b = n // per_class
    rest = n - b * per_class
    j = rest // per_residue
    i = rest - j * per_residue
    tail = n - full * per_class
    jt = tail // halo
    it = tail - jt * halo + per_residue - halo
    at_tail = b >= full
    return jnp.where(at_tail, jt, j), jnp.where(at_tail, it, i), b


def near_kernel(sp_ref, slot_ref, q_ref, kv0_ref, s1_ref, r1_ref, r2_ref, o0_ref, l0_ref, o1_ref, l1_ref):
    rows = kv0_ref.shape[0]
    sp = sp_ref[0]
    per_class = rows // CLASSES
    per_residue = rows // WIDE_DILATION
    halo = STEPS // WIDE_DILATION
    c, j, i = position_of_row(iota((rows, rows + STEPS), 0), rows)
    tq = 16 * i + 4 * j + c
    n = iota((rows, rows + STEPS), 1)
    c, j, i = position_of_row(n, rows)
    tail = n - rows
    r = tail // halo
    it = tail - r * halo + per_residue - halo
    t_tail = 16 * it + 4 * (r % 4) + r // 4 - rows
    is_tail = n >= rows
    tk = jnp.where(is_tail, t_tail, 16 * i + 4 * j + c)
    bias = bias_of(tq - tk, jnp.logical_or(jnp.logical_not(is_tail), sp >= 1), slope_of(0, slot_ref[0]))
    keys = jnp.concatenate([kv0_ref[...], r1_ref[0:STEPS, :]], axis=0)
    scores = dot(q_ref[:, 0:64], keys[:, 0:64], NT) + bias
    p, l = softmax_pieces(scores)
    o0_ref[...] = dot(p, keys[:, 64:128], NN)
    l0_ref[...] = l
    n_keys = 2 * per_class + STEPS // CLASSES
    q_row = iota((per_class, n_keys), 0)
    jq = q_row // per_residue
    iq = q_row - jq * per_residue
    jk, ik, b = key_rows(rows, n_keys, True)
    bias = bias_of(4 * (iq - ik) + jq - jk + per_class * b, b <= sp, slope_of(1, slot_ref[0]))
    for c in range(CLASSES):
        lo = STEPS + c * per_class
        keys = jnp.concatenate(
            [s1_ref[lo : lo + per_class, :], r1_ref[lo : lo + per_class, :], r2_ref[c * 32 : (c + 1) * 32, :]], axis=0
        )
        q = q_ref[c * per_class : (c + 1) * per_class, 64:128]
        p, l = softmax_pieces(dot(q, keys[:, 0:64], NT) + bias)
        o1_ref[c * per_class : (c + 1) * per_class, :] = dot(p, keys[:, 64:128], NN)
        l1_ref[c * per_class : (c + 1) * per_class, :] = l


def wide_kernel(sp_ref, slot_ref, q_ref, s3_ref, r1_ref, r2_ref, r3_ref, r4_ref, o0_ref, l0_ref, o1_ref, l1_ref, mix_ref, lw_ref, mixed_ref, l_ref):
    rows = s3_ref.shape[0]
    sp = sp_ref[0]
    per_class = rows // CLASSES
    per_residue = rows // WIDE_DILATION
    n_keys = 6 * per_class + STEPS // CLASSES
    q_row = iota((per_class, n_keys), 0)
    jq = q_row // per_residue
    iq = q_row - jq * per_residue
    jk, ik, b = key_rows(rows, n_keys, True)
    bias = bias_of(iq - ik + per_residue * b, (jq == jk) & (b <= sp), slope_of(2, slot_ref[0]))
    for c in range(CLASSES):
        lo = c * per_class
        run = pl.ds(lo, per_class)
        keys = jnp.concatenate(
            [
                s3_ref[run, :],
                r1_ref[pl.ds(STEPS + rows + lo, per_class), :],
                r2_ref[pl.ds(STEPS + lo, per_class), :],
                r3_ref[run, :],
                r4_ref[run, :],
                r4_ref[pl.ds(rows + lo, per_class), :],
                r4_ref[pl.ds(2 * rows + c * 32, 32), :],
            ],
            axis=0,
        )
        p, l2 = softmax_pieces(dot(q_ref[run, 128:192], keys[:, 0:64], NT) + bias)
        o2 = dot(p, keys[:, 64:128], NN)
        l0 = l0_ref[run, :]
        l1 = l1_ref[run, :]
        top = jnp.maximum(jnp.maximum(l0, l1), l2)
        lw = top + jnp.log(jnp.exp(l0 - top) + jnp.exp(l1 - top) + jnp.exp(l2 - top))
        mixed = (
            jnp.exp(l0 - lw) * o0_ref[run, :] + jnp.exp(l1 - lw) * o1_ref[run, :] + jnp.exp(l2 - lw) * o2
        )
        mixed_ref[run, :] = mixed.astype(jnp.bfloat16)
        l_ref[run, :] = lw
    pick = to_class_order(rows)
    mix = dot(mixed_ref[...], pick.astype(jnp.bfloat16), TN).astype(jnp.bfloat16)
    for n in range(mix_ref.shape[0]):
        mix_ref[n] = mix
    lw_ref[...] = jnp.sum(jnp.where(pick, l_ref[...], 0.0), axis=0, keepdims=True)


VMEM = pl.BlockSpec(memory_space=pltpu.VMEM)
SMEM = pl.BlockSpec(memory_space=pltpu.SMEM)
HBM = pl.BlockSpec(memory_space=pltpu.HBM)


def call(body, operands, outs, specs=None, scratch=()):
    return pl.pallas_call(
        body,
        in_specs=specs or [VMEM] * len(operands),
        out_specs=[VMEM] * len(outs),
        out_shape=[jax.ShapeDtypeStruct(s, d) for s, d in outs],
        scratch_shapes=list(scratch),
        compiler_params=pltpu.CompilerParams(vmem_limit_bytes=20 * 2**20),
    )(*operands)


def in_hbm(value):
    return pltpu.with_memory_space_constraint(value, pltpu.HBM)


def from_behind(value, by):
    devices = lax.axis_size("sp")
    return lax.ppermute(value, "sp", [(i, i + by) for i in range(devices - by)])


def layer(tokens, norm_gain, w_query, w_key, w_value, w_out):
    rows, width = tokens.shape
    bf16, f32 = jnp.bfloat16, jnp.float32
    sp = lax.axis_index("sp").reshape(1)
    slot = lax.axis_index("tp").reshape(1)
    kv0, s1, s2, s3, normed = call(
        project_kernel,
        (in_hbm(tokens), in_hbm(norm_gain.reshape(1, -1)), in_hbm(w_key), in_hbm(w_value)),
        [
            ((rows, 128), bf16),
            ((STEPS + 2 * rows, 128), bf16),
            ((STEPS + rows, 128), bf16),
            ((rows, 128), bf16),
            ((rows, width), bf16),
        ],
        specs=[HBM] * 4,
        scratch=[
            pltpu.VMEM((rows, width), bf16),
            pltpu.VMEM((1, width), f32),
            pltpu.VMEM((GROUPS * 128, width), bf16),
            pltpu.SemaphoreType.DMA((rows // CHUNK + 2 * GROUPS + 1,)),
        ],
    )
    r2 = from_behind(s2, 2)
    r1 = from_behind(s1, 1)
    r3 = from_behind(s3, 3)
    (q,) = call(query_kernel, (normed, w_query), [((rows, GROUPS * HEAD_DIM), bf16)])
    (s4,) = call(relay_kernel, (s3, r1, r2), [((STEPS + 2 * rows, 128), bf16)])
    r4 = from_behind(s4, 4)
    o0, l0, o1, l1 = call(
        near_kernel,
        (sp, slot, q, kv0, s1, r1, r2),
        [((rows, HEAD_DIM), f32), ((rows, 1), f32), ((rows, HEAD_DIM), f32), ((rows, 1), f32)],
        specs=[SMEM] * 2 + [VMEM] * 5,
    )
    devices = lax.axis_size("tp")
    mix, log_weight = call(
        wide_kernel,
        (sp, slot, q, s3, r1, r2, r3, r4, o0, l0, o1, l1),
        [((devices, HEAD_DIM, rows), bf16), ((1, rows), f32)],
        specs=[SMEM] * 2 + [VMEM] * 10,
        scratch=[pltpu.VMEM((rows, HEAD_DIM), bf16), pltpu.VMEM((rows, 1), f32)],
    )
    everyone = lax.all_to_all(mix, "tp", 0, 0, tiled=True)
    projected = dot(everyone.reshape(devices * HEAD_DIM, rows), w_out, TN)
    return projected.astype(bf16), log_weight


def solution(mesh):
    in_specs = (P("sp", None), P(), P(None, "tp", None), P(None, "tp", None), P(None, "tp", None), P(None, "tp"))
    out_specs = (P("sp", "tp"), P("tp", "sp"))
    return jax.shard_map(layer, mesh=mesh, in_specs=in_specs, out_specs=out_specs, check_vma=False)
```

```python
import jax
import jax.numpy as jnp
from jax import lax
from jax.experimental import pallas as pl
from jax.experimental.pallas import tpu as pltpu
from jax.sharding import PartitionSpec as P


HEAD_DIM = 64
SLOTS = 8
STEPS = 128
GROUPS = 3
WIDE_DILATION = 16
NEG_BIG = -1e30

CLASSES = 4
PAIR = 2 * HEAD_DIM
CHUNK = 128
HALO = STEPS // WIDE_DILATION
NT = (((1,), (1,)), ((), ()))
NN = (((1,), (0,)), ((), ()))
TN = (((0,), (0,)), ((), ()))


def dot(a, b, dims):
    return lax.dot_general(a, b, dims, preferred_element_type=jnp.float32)


def line(length, dim):
    return lax.broadcasted_iota(jnp.int32, (length, 1) if dim == 0 else (1, length), dim)


def split(n, size):
    q = jnp.zeros_like(n)
    for k in range(1, 32):
        q = q + (n >= k * size).astype(jnp.int32)
    return q, n - q * size


def run_of_class(per_class, dim):
    return split(line(per_class, dim), per_class // CLASSES)


def run_of_halo(rows_per_residue, dim):
    j, i = split(line(STEPS // CLASSES, dim), HALO)
    return j, i + rows_per_residue - HALO


def positions(rows, dim):
    j, i = run_of_class(rows // CLASSES, dim)
    return jnp.concatenate([16 * i + 4 * j + c for c in range(CLASSES)], axis=dim)


def to_class_order(rows):
    return positions(rows, 0) == line(rows, 1)


def halo_rows(rows):
    per_residue = rows // WIDE_DILATION
    return [r * per_residue + per_residue - HALO for r in range(WIDE_DILATION)]


def project_kernel(
    tokens_hbm, gain_hbm, wk_hbm, wv_hbm, kv0_ref, s1_ref, s3_ref, s6_ref, normed_ref, x_ref, gain_ref, w_ref, sem
):
    rows = x_ref.shape[0]
    chunks = rows // CHUNK
    gain_load = pltpu.make_async_copy(gain_hbm, gain_ref, sem.at[chunks + 2 * GROUPS])
    gain_load.start()
    loads = [
        pltpu.make_async_copy(tokens_hbm.at[pl.ds(n * CHUNK, CHUNK)], x_ref.at[pl.ds(n * CHUNK, CHUNK)], sem.at[n])
        for n in range(chunks)
    ]
    for g in range(GROUPS):
        at = chunks + 2 * g
        loads.append(pltpu.make_async_copy(wk_hbm.at[g], w_ref.at[pl.ds(g * PAIR, HEAD_DIM)], sem.at[at]))
        loads.append(
            pltpu.make_async_copy(wv_hbm.at[g], w_ref.at[pl.ds(g * PAIR + HEAD_DIM, HEAD_DIM)], sem.at[at + 1])
        )
    for load in loads:
        load.start()
    pick = to_class_order(rows).astype(jnp.bfloat16)
    gain_load.wait()
    gain = gain_ref[...]
    for n in range(chunks):
        loads[n].wait()
        run = pl.ds(n * CHUNK, CHUNK)
        x = x_ref[run, :].astype(jnp.float32)
        mean = jnp.mean(x * x, axis=-1, keepdims=True)
        normed_ref[run, :] = (x * lax.rsqrt(mean + 1e-6) * gain).astype(jnp.bfloat16)
    for load in loads[chunks:]:
        load.wait()
    kv = dot(normed_ref[...], w_ref[...], NT).astype(jnp.bfloat16)
    kv = dot(pick, kv, NN).astype(jnp.bfloat16)
    kv0_ref[...] = kv[:, 0:PAIR]
    s1_ref[STEPS : STEPS + rows, :] = kv[:, PAIR : 2 * PAIR]
    s1_ref[STEPS + rows : STEPS + 2 * rows, :] = kv[:, 2 * PAIR : 3 * PAIR]
    s3_ref[...] = kv[:, 2 * PAIR : 3 * PAIR]
    for r, lo in enumerate(halo_rows(rows)):
        s1_ref[r * HALO : (r + 1) * HALO, :] = kv[lo : lo + HALO, 0:PAIR]
        s6_ref[r * HALO : (r + 1) * HALO, :] = kv[lo : lo + HALO, 2 * PAIR : 3 * PAIR]


def query_kernel(normed_ref, wq_ref, q_ref):
    rows = normed_ref.shape[0]
    wq = wq_ref[...].reshape(GROUPS * HEAD_DIM, -1)
    q = (dot(normed_ref[...], wq, NT).astype(jnp.bfloat16) * jnp.bfloat16(0.125)).astype(jnp.bfloat16)
    q_ref[...] = dot(to_class_order(rows).astype(jnp.bfloat16), q, NN).astype(jnp.bfloat16)


def relay_kernel(s3_ref, r1_ref, s4_ref, s1b_ref):
    rows = s3_ref.shape[0]
    before = r1_ref[STEPS + rows : STEPS + 2 * rows, :]
    s4_ref[0:rows, :] = s3_ref[...]
    s4_ref[rows : 2 * rows, :] = before
    s1b_ref[STEPS : STEPS + rows, :] = before
    for r, lo in enumerate(halo_rows(rows)):
        s1b_ref[r * HALO : (r + 1) * HALO, :] = r1_ref[STEPS + lo : STEPS + lo + HALO, :]


def slope_of(group, slot):
    n = jnp.full((1, 1), group * SLOTS + 1, jnp.int32) + slot
    return jnp.exp2(-8.0 * n.astype(jnp.float32) / (GROUPS * SLOTS))


def bias_of(distance, valid, slope):
    ok = valid & (distance >= 0) & (distance <= STEPS)
    return jnp.where(ok, -slope * distance.astype(jnp.float32), NEG_BIG)


def softmax_pieces(scores):
    top = jnp.max(scores, axis=-1, keepdims=True)
    e = jnp.exp(scores - top)
    total = jnp.sum(e, axis=-1, keepdims=True)
    return (e * (1.0 / total)).astype(jnp.bfloat16), top + jnp.log(total)


def wide_bias(rows, blocks, sp, slope, halo_block=None):
    per_class, per_residue = rows // CLASSES, rows // WIDE_DILATION
    jq, iq = run_of_class(per_class, 0)
    jk, ik = run_of_class(per_class, 1)
    js, at, ok = [], [], []
    for b in blocks:
        js.append(jk)
        at.append(ik - per_residue * b)
        ok.append(jnp.full_like(jk, b) <= sp)
    if halo_block is not None:
        jh, ih = run_of_halo(per_residue, 1)
        js.append(jh)
        at.append(ih - per_residue * halo_block)
        ok.append(jnp.full_like(jh, halo_block) <= sp)
    js, at = jnp.concatenate(js, axis=1), jnp.concatenate(at, axis=1)
    ok = jnp.concatenate([o.astype(jnp.int32) for o in ok], axis=1) > 0
    return bias_of(iq - at, (jq == js) & ok, slope)


def early_kernel(sp_ref, slot_ref, q_ref, kv0_ref, s3_ref, r1_ref, r3_ref, o0_ref, l0_ref, e_ref, top_ref, sum_ref):
    rows = kv0_ref.shape[0]
    sp, slot = sp_ref[0], slot_ref[0]
    per_class, per_residue = rows // CLASSES, rows // WIDE_DILATION
    jh, ih = run_of_halo(per_residue, 1)
    tail = jnp.concatenate([16 * ih + 4 * jh + c - rows for c in range(CLASSES)], axis=1)
    tk = jnp.concatenate([positions(rows, 1), tail], axis=1)
    bias = bias_of(positions(rows, 0) - tk, (tk >= 0) | (sp >= 1), slope_of(0, slot))
    keys = jnp.concatenate([kv0_ref[...], r1_ref[0:STEPS, :]], axis=0)
    p, l = softmax_pieces(dot(q_ref[:, 0:HEAD_DIM], keys[:, 0:HEAD_DIM], NT) + bias)
    o0_ref[...] = dot(p, keys[:, HEAD_DIM:PAIR], NN)
    l0_ref[...] = l
    bias = wide_bias(rows, (0, 1, 3), sp, slope_of(2, slot))
    for c in range(CLASSES):
        lo = c * per_class
        run = pl.ds(lo, per_class)
        keys = jnp.concatenate([s3_ref[run, :], r1_ref[pl.ds(STEPS + rows + lo, per_class), :], r3_ref[run, :]], axis=0)
        scores = dot(q_ref[run, 2 * HEAD_DIM : 3 * HEAD_DIM], keys[:, 0:HEAD_DIM], NT) + bias
        top = jnp.max(scores, axis=-1, keepdims=True)
        e = jnp.exp(scores - top)
        e_ref[run, :] = e
        top_ref[run, :] = top
        sum_ref[run, :] = jnp.sum(e, axis=-1, keepdims=True)


def late_kernel(
    sp_ref, slot_ref, q_ref, s1_ref, s3_ref, r1_ref, r3_ref, r1b_ref, r4_ref, r6_ref, o0_ref, l0_ref, e_ref, top_ref,
    sum_ref, mix_ref, lw_ref, mixed_ref, l_ref,
):
    rows = s3_ref.shape[0]
    sp, slot = sp_ref[0], slot_ref[0]
    per_class, per_residue = rows // CLASSES, rows // WIDE_DILATION
    jq, iq = run_of_class(per_class, 0)
    jk, ik = run_of_class(per_class, 1)
    jh, ih = run_of_halo(per_residue, 1)
    own = 4 * ik + jk
    tk = jnp.concatenate([own, own - per_class, 4 * ih + jh - 2 * per_class], axis=1)
    near = jnp.concatenate(
        [jnp.zeros_like(own), jnp.full_like(own, 1), jnp.full_like(jh, 2)], axis=1
    )
    bias1 = bias_of(4 * iq + jq - tk, near <= sp, slope_of(1, slot))
    bias2 = wide_bias(rows, (2, 4, 5), sp, slope_of(2, slot), halo_block=6)
    halo = STEPS // CLASSES
    for c in range(CLASSES):
        lo = c * per_class
        run = pl.ds(lo, per_class)
        keys = jnp.concatenate(
            [s1_ref[pl.ds(STEPS + lo, per_class), :], r1_ref[pl.ds(STEPS + lo, per_class), :], r1b_ref[pl.ds(c * halo, halo), :]],
            axis=0,
        )
        p, l1 = softmax_pieces(dot(q_ref[run, HEAD_DIM : 2 * HEAD_DIM], keys[:, 0:HEAD_DIM], NT) + bias1)
        o1 = dot(p, keys[:, HEAD_DIM:PAIR], NN)
        keys = jnp.concatenate(
            [
                r1b_ref[pl.ds(STEPS + lo, per_class), :],
                r4_ref[run, :],
                r4_ref[pl.ds(rows + lo, per_class), :],
                r6_ref[pl.ds(c * halo, halo), :],
            ],
            axis=0,
        )
        scores = dot(q_ref[run, 2 * HEAD_DIM : 3 * HEAD_DIM], keys[:, 0:HEAD_DIM], NT) + bias2
        top0 = top_ref[run, :]
        top = jnp.maximum(top0, jnp.max(scores, axis=-1, keepdims=True))
        e = jnp.exp(scores - top)
        shrink = jnp.exp(top0 - top)
        total = sum_ref[run, :] * shrink + jnp.sum(e, axis=-1, keepdims=True)
        scale = 1.0 / total
        l2 = top + jnp.log(total)
        early = jnp.concatenate(
            [s3_ref[run, HEAD_DIM:PAIR], r1_ref[pl.ds(STEPS + rows + lo, per_class), HEAD_DIM:PAIR], r3_ref[run, HEAD_DIM:PAIR]],
            axis=0,
        )
        o2 = dot((e * scale).astype(jnp.bfloat16), keys[:, HEAD_DIM:PAIR], NN)
        o2 = o2 + dot((e_ref[run, :] * (shrink * scale)).astype(jnp.bfloat16), early, NN)
        l0 = l0_ref[run, :]
        top = jnp.maximum(jnp.maximum(l0, l1), l2)
        lw = top + jnp.log(jnp.exp(l0 - top) + jnp.exp(l1 - top) + jnp.exp(l2 - top))
        mixed = jnp.exp(l0 - lw) * o0_ref[run, :] + jnp.exp(l1 - lw) * o1 + jnp.exp(l2 - lw) * o2
        mixed_ref[run, :] = mixed.astype(jnp.bfloat16)
        l_ref[run, :] = lw
    pick = to_class_order(rows)
    mix = dot(mixed_ref[...], pick.astype(jnp.bfloat16), TN).astype(jnp.bfloat16)
    for n in range(mix_ref.shape[0]):
        mix_ref[n] = mix
    lw_ref[...] = jnp.sum(jnp.where(pick, l_ref[...], 0.0), axis=0, keepdims=True)


VMEM = pl.BlockSpec(memory_space=pltpu.VMEM)
SMEM = pl.BlockSpec(memory_space=pltpu.SMEM)
HBM = pl.BlockSpec(memory_space=pltpu.HBM)


def call(body, operands, outs, specs=None, scratch=()):
    return pl.pallas_call(
        body,
        in_specs=specs or [VMEM] * len(operands),
        out_specs=[VMEM] * len(outs),
        out_shape=[jax.ShapeDtypeStruct(s, d) for s, d in outs],
        scratch_shapes=list(scratch),
        compiler_params=pltpu.CompilerParams(vmem_limit_bytes=20 * 2**20),
    )(*operands)


def in_hbm(value):
    return pltpu.with_memory_space_constraint(value, pltpu.HBM)


def from_behind(value, by):
    devices = lax.axis_size("sp")
    return lax.ppermute(value, "sp", [(i, i + by) for i in range(devices - by)])


def layer(tokens, norm_gain, w_query, w_key, w_value, w_out):
    rows, width = tokens.shape
    bf16, f32 = jnp.bfloat16, jnp.float32
    sp = lax.axis_index("sp").reshape(1)
    slot = lax.axis_index("tp").reshape(1)
    kv0, s1, s3, s6, normed = call(
        project_kernel,
        (in_hbm(tokens), in_hbm(norm_gain.reshape(1, -1)), in_hbm(w_key), in_hbm(w_value)),
        [
            ((rows, PAIR), bf16),
            ((STEPS + 2 * rows, PAIR), bf16),
            ((rows, PAIR), bf16),
            ((STEPS, PAIR), bf16),
            ((rows, width), bf16),
        ],
        specs=[HBM] * 4,
        scratch=[
            pltpu.VMEM((rows, width), bf16),
            pltpu.VMEM((1, width), f32),
            pltpu.VMEM((GROUPS * PAIR, width), bf16),
            pltpu.SemaphoreType.DMA((rows // CHUNK + 2 * GROUPS + 1,)),
        ],
    )
    r1 = from_behind(s1, 1)
    r3 = from_behind(s3, 3)
    r6 = from_behind(s6, 6)
    (q,) = call(query_kernel, (normed, w_query), [((rows, GROUPS * HEAD_DIM), bf16)])
    s4, s1b = call(relay_kernel, (s3, r1), [((2 * rows, PAIR), bf16), ((STEPS + rows, PAIR), bf16)])
    r4 = from_behind(s4, 4)
    r1b = from_behind(s1b, 1)
    o0, l0, e, top, total = call(
        early_kernel,
        (sp, slot, q, kv0, s3, r1, r3),
        [
            ((rows, HEAD_DIM), f32),
            ((rows, 1), f32),
            ((rows, 3 * rows // CLASSES), f32),
            ((rows, 1), f32),
            ((rows, 1), f32),
        ],
        specs=[SMEM] * 2 + [VMEM] * 5,
    )
    devices = lax.axis_size("tp")
    mix, log_weight = call(
        late_kernel,
        (sp, slot, q, s1, s3, r1, r3, r1b, r4, r6, o0, l0, e, top, total),
        [((devices, HEAD_DIM, rows), bf16), ((1, rows), f32)],
        specs=[SMEM] * 2 + [VMEM] * 13,
        scratch=[pltpu.VMEM((rows, HEAD_DIM), bf16), pltpu.VMEM((rows, 1), f32)],
    )
    everyone = lax.all_to_all(mix, "tp", 0, 0, tiled=True)
    projected = dot(everyone.reshape(devices * HEAD_DIM, rows), w_out, TN)
    return projected.astype(bf16), log_weight


def solution(mesh):
    in_specs = (P("sp", None), P(), P(None, "tp", None), P(None, "tp", None), P(None, "tp", None), P(None, "tp"))
    out_specs = (P("sp", "tp"), P("tp", "sp"))
    return jax.shard_map(layer, mesh=mesh, in_specs=in_specs, out_specs=out_specs, check_vma=False)
```

```python
import jax
import jax.numpy as jnp
from jax import lax
from jax.experimental import pallas as pl
from jax.experimental.pallas import tpu as pltpu
from jax.sharding import PartitionSpec as P


HEAD_DIM = 64
SLOTS = 8
STEPS = 128
GROUPS = 3
WIDE_DILATION = 16
NEG_BIG = -1e30

CLASSES = 4
PAIR = 2 * HEAD_DIM
CHUNK = 128
HALO = STEPS // WIDE_DILATION
NT = (((1,), (1,)), ((), ()))
NN = (((1,), (0,)), ((), ()))
TN = (((0,), (0,)), ((), ()))


def dot(a, b, dims):
    return lax.dot_general(a, b, dims, preferred_element_type=jnp.float32)


def line(length, dim):
    return lax.broadcasted_iota(jnp.int32, (length, 1) if dim == 0 else (1, length), dim)


def split(n, size):
    q = jnp.zeros_like(n)
    for k in range(1, 32):
        q = q + (n >= k * size).astype(jnp.int32)
    return q, n - q * size


def run_of_class(per_class, dim):
    return split(line(per_class, dim), per_class // CLASSES)


def run_of_halo(rows_per_residue, dim):
    j, i = split(line(STEPS // CLASSES, dim), HALO)
    return j, i + rows_per_residue - HALO


def positions(rows, dim):
    j, i = run_of_class(rows // CLASSES, dim)
    return jnp.concatenate([16 * i + 4 * j + c for c in range(CLASSES)], axis=dim)


def to_class_order(rows):
    return positions(rows, 0) == line(rows, 1)


def halo_rows(rows):
    per_residue = rows // WIDE_DILATION
    return [r * per_residue + per_residue - HALO for r in range(WIDE_DILATION)]


def project_kernel(
    tokens_hbm, gain_hbm, wk_hbm, wv_hbm, kv0_ref, s1_ref, s2_ref, s3_ref, normed_ref, x_ref, gain_ref, w_ref, sem
):
    rows = x_ref.shape[0]
    chunks = rows // CHUNK
    gain_load = pltpu.make_async_copy(gain_hbm, gain_ref, sem.at[chunks + 2 * GROUPS])
    gain_load.start()
    loads = [
        pltpu.make_async_copy(tokens_hbm.at[pl.ds(n * CHUNK, CHUNK)], x_ref.at[pl.ds(n * CHUNK, CHUNK)], sem.at[n])
        for n in range(chunks)
    ]
    for g in range(GROUPS):
        at = chunks + 2 * g
        loads.append(pltpu.make_async_copy(wk_hbm.at[g], w_ref.at[pl.ds(g * PAIR, HEAD_DIM)], sem.at[at]))
        loads.append(
            pltpu.make_async_copy(wv_hbm.at[g], w_ref.at[pl.ds(g * PAIR + HEAD_DIM, HEAD_DIM)], sem.at[at + 1])
        )
    for load in loads:
        load.start()
    pick = to_class_order(rows).astype(jnp.bfloat16)
    gain_load.wait()
    gain = gain_ref[...]
    for n in range(chunks):
        loads[n].wait()
        run = pl.ds(n * CHUNK, CHUNK)
        x = x_ref[run, :].astype(jnp.float32)
        mean = jnp.mean(x * x, axis=-1, keepdims=True)
        normed_ref[run, :] = (x * lax.rsqrt(mean + 1e-6) * gain).astype(jnp.bfloat16)
    for load in loads[chunks:]:
        load.wait()
    kv = dot(normed_ref[...], w_ref[...], NT).astype(jnp.bfloat16)
    kv = dot(pick, kv, NN).astype(jnp.bfloat16)
    kv0_ref[...] = kv[:, 0:PAIR]
    s1_ref[STEPS : STEPS + rows, :] = kv[:, PAIR : 2 * PAIR]
    s1_ref[STEPS + rows : STEPS + 2 * rows, :] = kv[:, 2 * PAIR : 3 * PAIR]
    s2_ref[STEPS : STEPS + rows, :] = kv[:, 2 * PAIR : 3 * PAIR]
    s3_ref[...] = kv[:, 2 * PAIR : 3 * PAIR]
    for r, lo in enumerate(halo_rows(rows)):
        s1_ref[r * HALO : (r + 1) * HALO, :] = kv[lo : lo + HALO, 0:PAIR]
        s2_ref[r * HALO : (r + 1) * HALO, :] = kv[lo : lo + HALO, PAIR : 2 * PAIR]


def query_kernel(normed_ref, wq_ref, q_ref):
    rows = normed_ref.shape[0]
    wq = wq_ref[...].reshape(GROUPS * HEAD_DIM, -1)
    q = (dot(normed_ref[...], wq, NT).astype(jnp.bfloat16) * jnp.bfloat16(0.125)).astype(jnp.bfloat16)
    q_ref[...] = dot(to_class_order(rows).astype(jnp.bfloat16), q, NN).astype(jnp.bfloat16)


def relay_kernel(s3_ref, r1_ref, r2_ref, s4_ref):
    rows = s3_ref.shape[0]
    s4_ref[0:rows, :] = s3_ref[...]
    s4_ref[rows : 2 * rows, :] = r1_ref[STEPS + rows : STEPS + 2 * rows, :]
    for r, lo in enumerate(halo_rows(rows)):
        at = 2 * rows + r * HALO
        s4_ref[at : at + HALO, :] = r2_ref[STEPS + lo : STEPS + lo + HALO, :]


def slope_of(group, slot):
    n = jnp.full((1, 1), group * SLOTS + 1, jnp.int32) + slot
    return jnp.exp2(-8.0 * n.astype(jnp.float32) / (GROUPS * SLOTS))


def bias_of(distance, valid, slope):
    ok = valid & (distance >= 0) & (distance <= STEPS)
    return jnp.where(ok, -slope * distance.astype(jnp.float32), NEG_BIG)


def softmax_pieces(scores):
    top = jnp.max(scores, axis=-1, keepdims=True)
    e = jnp.exp(scores - top)
    total = jnp.sum(e, axis=-1, keepdims=True)
    return (e * (1.0 / total)).astype(jnp.bfloat16), top + jnp.log(total)


def wide_bias(rows, blocks, sp, slope, halo_block=None):
    per_class, per_residue = rows // CLASSES, rows // WIDE_DILATION
    jq, iq = run_of_class(per_class, 0)
    jk, ik = run_of_class(per_class, 1)
    js, at, ok = [], [], []
    for b in blocks:
        js.append(jk)
        at.append(ik - per_residue * b)
        ok.append(jnp.full_like(jk, b) <= sp)
    if halo_block is not None:
        jh, ih = run_of_halo(per_residue, 1)
        js.append(jh)
        at.append(ih - per_residue * halo_block)
        ok.append(jnp.full_like(jh, halo_block) <= sp)
    js, at = jnp.concatenate(js, axis=1), jnp.concatenate(at, axis=1)
    ok = jnp.concatenate([o.astype(jnp.int32) for o in ok], axis=1) > 0
    return bias_of(iq - at, (jq == js) & ok, slope)


def early_kernel(
    sp_ref, slot_ref, q_ref, kv0_ref, s1_ref, s3_ref, r1_ref, r2_ref, r3_ref, o_ref, l_ref, e_ref, top_ref, sum_ref
):
    rows = kv0_ref.shape[0]
    sp, slot = sp_ref[0], slot_ref[0]
    per_class, per_residue = rows // CLASSES, rows // WIDE_DILATION
    runs = [pl.ds(c * per_class, per_class) for c in range(CLASSES)]
    jh, ih = run_of_halo(per_residue, 1)
    tail = jnp.concatenate([16 * ih + 4 * jh + c - rows for c in range(CLASSES)], axis=1)
    tk = jnp.concatenate([positions(rows, 1), tail], axis=1)
    bias = bias_of(positions(rows, 0) - tk, (tk >= 0) | (sp >= 1), slope_of(0, slot))
    keys = jnp.concatenate([kv0_ref[...], r1_ref[0:STEPS, :]], axis=0)
    p, l0 = softmax_pieces(dot(q_ref[:, 0:HEAD_DIM], keys[:, 0:HEAD_DIM], NT) + bias)
    o0 = dot(p, keys[:, HEAD_DIM:PAIR], NN)
    jq, iq = run_of_class(per_class, 0)
    jk, ik = run_of_class(per_class, 1)
    own = 4 * ik + jk
    tk = jnp.concatenate([own, own - per_class, 4 * ih + jh - 2 * per_class], axis=1)
    block = jnp.concatenate([jnp.zeros_like(own), jnp.full_like(own, 1), jnp.full_like(jh, 2)], axis=1)
    bias = bias_of(4 * iq + jq - tk, block <= sp, slope_of(1, slot))
    halo = STEPS // CLASSES
    keys = [
        jnp.concatenate(
            [
                s1_ref[pl.ds(STEPS + c * per_class, per_class), :],
                r1_ref[pl.ds(STEPS + c * per_class, per_class), :],
                r2_ref[pl.ds(c * halo, halo), :],
            ],
            axis=0,
        )
        for c in range(CLASSES)
    ]
    scores = [dot(q_ref[runs[c], HEAD_DIM : 2 * HEAD_DIM], keys[c][:, 0:HEAD_DIM], NT) + bias for c in range(CLASSES)]
    p, l1 = softmax_pieces(jnp.concatenate(scores, axis=0))
    o1 = [
        dot(p[c * per_class : (c + 1) * per_class], keys[c][:, HEAD_DIM:PAIR], NN) for c in range(CLASSES)
    ]
    top = jnp.maximum(l0, l1)
    w0, w1 = jnp.exp(l0 - top), jnp.exp(l1 - top)
    both = w0 + w1
    l_ref[...] = top + jnp.log(both)
    both = 1.0 / both
    o_ref[...] = (w0 * both) * o0 + (w1 * both) * jnp.concatenate(o1, axis=0)
    bias = wide_bias(rows, (0, 1, 2, 3), sp, slope_of(2, slot))
    scores = []
    for c in range(CLASSES):
        lo = c * per_class
        keys = jnp.concatenate(
            [
                s3_ref[runs[c], 0:HEAD_DIM],
                r1_ref[pl.ds(STEPS + rows + lo, per_class), 0:HEAD_DIM],
                r2_ref[pl.ds(STEPS + lo, per_class), 0:HEAD_DIM],
                r3_ref[runs[c], 0:HEAD_DIM],
            ],
            axis=0,
        )
        scores.append(dot(q_ref[runs[c], 2 * HEAD_DIM : 3 * HEAD_DIM], keys, NT) + bias)
    scores = jnp.concatenate(scores, axis=0)
    top = jnp.max(scores, axis=-1, keepdims=True)
    e = jnp.exp(scores - top)
    e_ref[...] = e
    top_ref[...] = top
    sum_ref[...] = jnp.sum(e, axis=-1, keepdims=True)


def late_kernel(
    sp_ref, slot_ref, q_ref, s3_ref, r1_ref, r2_ref, r3_ref, r4_ref, o_ref, l_ref, e_ref, top_ref, sum_ref, mix_ref, lw_ref
):
    rows = s3_ref.shape[0]
    sp, slot = sp_ref[0], slot_ref[0]
    per_class = rows // CLASSES
    halo = STEPS // CLASSES
    runs = [pl.ds(c * per_class, per_class) for c in range(CLASSES)]
    bias = wide_bias(rows, (4, 5), sp, slope_of(2, slot), halo_block=6)
    keys = [
        jnp.concatenate(
            [r4_ref[runs[c], :], r4_ref[pl.ds(rows + c * per_class, per_class), :], r4_ref[pl.ds(2 * rows + c * halo, halo), :]],
            axis=0,
        )
        for c in range(CLASSES)
    ]
    scores = jnp.concatenate(
        [dot(q_ref[runs[c], 2 * HEAD_DIM : 3 * HEAD_DIM], keys[c][:, 0:HEAD_DIM], NT) + bias for c in range(CLASSES)], axis=0
    )
    top0 = top_ref[...]
    top = jnp.maximum(top0, jnp.max(scores, axis=-1, keepdims=True))
    e = jnp.exp(scores - top)
    shrink = jnp.exp(top0 - top)
    total = sum_ref[...] * shrink + jnp.sum(e, axis=-1, keepdims=True)
    scale = 1.0 / total
    l2 = top + jnp.log(total)
    p = (e * scale).astype(jnp.bfloat16)
    p_early = (e_ref[...] * (shrink * scale)).astype(jnp.bfloat16)
    out = []
    for c in range(CLASSES):
        lo = c * per_class
        early = jnp.concatenate(
            [
                s3_ref[runs[c], HEAD_DIM:PAIR],
                r1_ref[pl.ds(STEPS + rows + lo, per_class), HEAD_DIM:PAIR],
                r2_ref[pl.ds(STEPS + lo, per_class), HEAD_DIM:PAIR],
                r3_ref[runs[c], HEAD_DIM:PAIR],
            ],
            axis=0,
        )
        out.append(
            dot(p_early[lo : lo + per_class], early, NN) + dot(p[lo : lo + per_class], keys[c][:, HEAD_DIM:PAIR], NN)
        )
    l01 = l_ref[...]
    top = jnp.maximum(l01, l2)
    w01, w2 = jnp.exp(l01 - top), jnp.exp(l2 - top)
    both = w01 + w2
    lw_ref[...] = top + jnp.log(both)
    both = 1.0 / both
    mixed = ((w01 * both) * o_ref[...] + (w2 * both) * jnp.concatenate(out, axis=0)).astype(jnp.bfloat16)
    mix = dot(mixed, to_class_order(rows).astype(jnp.bfloat16), TN).astype(jnp.bfloat16)
    for n in range(mix_ref.shape[0]):
        mix_ref[n] = mix


def slots_of(core, w_ref):
    return jnp.concatenate([w_ref[2 * x + core] for x in range(SLOTS // 2)], axis=0)


def own_slots_kernel(slot_ref, mix_ref, w_ref, lw_ref, acc_ref, log_weight_ref):
    rows = lw_ref.shape[0]
    mixed = mix_ref[...].reshape(-1, rows)
    acc_ref[...] = dot(mixed, slots_of(slot_ref[0] % 2, w_ref), TN)
    log_weight_ref[...] = jnp.sum(jnp.where(to_class_order(rows), lw_ref[...], 0.0), axis=0, keepdims=True)


def other_slots_kernel(slot_ref, mix_ref, w_ref, acc_ref, out_ref):
    mixed = mix_ref[...].reshape(-1, acc_ref.shape[0])
    out_ref[...] = (acc_ref[...] + dot(mixed, slots_of(1 - slot_ref[0] % 2, w_ref), TN)).astype(jnp.bfloat16)


VMEM = pl.BlockSpec(memory_space=pltpu.VMEM)
SMEM = pl.BlockSpec(memory_space=pltpu.SMEM)
HBM = pl.BlockSpec(memory_space=pltpu.HBM)


def call(body, operands, outs, specs=None, scratch=()):
    return pl.pallas_call(
        body,
        in_specs=specs or [VMEM] * len(operands),
        out_specs=[VMEM] * len(outs),
        out_shape=[jax.ShapeDtypeStruct(s, d) for s, d in outs],
        scratch_shapes=list(scratch),
        compiler_params=pltpu.CompilerParams(vmem_limit_bytes=20 * 2**20),
    )(*operands)


def in_hbm(value):
    return pltpu.with_memory_space_constraint(value, pltpu.HBM)


def from_behind(value, by):
    devices = lax.axis_size("sp")
    return lax.ppermute(value, "sp", [(i, i + by) for i in range(devices - by)])


def layer(tokens, norm_gain, w_query, w_key, w_value, w_out):
    rows, width = tokens.shape
    bf16, f32 = jnp.bfloat16, jnp.float32
    sp = lax.axis_index("sp").reshape(1)
    slot = lax.axis_index("tp").reshape(1)
    kv0, s1, s2, s3, normed = call(
        project_kernel,
        (in_hbm(tokens), in_hbm(norm_gain.reshape(1, -1)), in_hbm(w_key), in_hbm(w_value)),
        [
            ((rows, PAIR), bf16),
            ((STEPS + 2 * rows, PAIR), bf16),
            ((STEPS + rows, PAIR), bf16),
            ((rows, PAIR), bf16),
            ((rows, width), bf16),
        ],
        specs=[HBM] * 4,
        scratch=[
            pltpu.VMEM((rows, width), bf16),
            pltpu.VMEM((1, width), f32),
            pltpu.VMEM((GROUPS * PAIR, width), bf16),
            pltpu.SemaphoreType.DMA((rows // CHUNK + 2 * GROUPS + 1,)),
        ],
    )
    r1 = from_behind(s1, 1)
    r2 = from_behind(s2, 2)
    r3 = from_behind(s3, 3)
    (q,) = call(query_kernel, (normed, w_query), [((rows, GROUPS * HEAD_DIM), bf16)])
    (s4,) = call(relay_kernel, (s3, r1, r2), [((STEPS + 2 * rows, PAIR), bf16)])
    r4 = from_behind(s4, 4)
    o, l, e, top, total = call(
        early_kernel,
        (sp, slot, q, kv0, s1, s3, r1, r2, r3),
        [((rows, HEAD_DIM), f32), ((rows, 1), f32), ((rows, rows), f32), ((rows, 1), f32), ((rows, 1), f32)],
        specs=[SMEM] * 2 + [VMEM] * 7,
    )
    devices = lax.axis_size("tp")
    mix, lw = call(
        late_kernel,
        (sp, slot, q, s3, r1, r2, r3, r4, o, l, e, top, total),
        [((devices // 2, HEAD_DIM, rows), bf16), ((rows, 1), f32)],
        specs=[SMEM] * 2 + [VMEM] * 11,
    )
    same_core = [[2 * x + core for x in range(devices // 2)] for core in range(2)]
    own = lax.all_to_all(mix, "tp", 0, 0, tiled=True, axis_index_groups=same_core)
    other = lax.ppermute(own, "tp", [(i, i ^ 1) for i in range(devices)])
    w = w_out.reshape(devices, HEAD_DIM, -1)
    acc, log_weight = call(
        own_slots_kernel, (slot, own, w, lw), [((rows, w.shape[2]), f32), ((1, rows), f32)], specs=[SMEM] + [VMEM] * 3
    )
    (projected,) = call(
        other_slots_kernel, (slot, other, w, acc), [((rows, w.shape[2]), bf16)], specs=[SMEM] + [VMEM] * 3
    )
    return projected, log_weight


def solution(mesh):
    in_specs = (P("sp", None), P(), P(None, "tp", None), P(None, "tp", None), P(None, "tp", None), P(None, "tp"))
    out_specs = (P("sp", "tp"), P("tp", "sp"))
    return jax.shard_map(layer, mesh=mesh, in_specs=in_specs, out_specs=out_specs, check_vma=False)
```

```python
import jax
import jax.numpy as jnp
from jax import lax
from jax.experimental import pallas as pl
from jax.experimental.pallas import tpu as pltpu
from jax.sharding import PartitionSpec as P


HEAD_DIM = 64
SLOTS = 8
STEPS = 128
GROUPS = 3
WIDE_DILATION = 16
NEG_BIG = -1e30

CLASSES = 4
PAIR = 2 * HEAD_DIM
CHUNK = 128
HALO = STEPS // WIDE_DILATION
NT = (((1,), (1,)), ((), ()))
NN = (((1,), (0,)), ((), ()))
TN = (((0,), (0,)), ((), ()))


def dot(a, b, dims):
    return lax.dot_general(a, b, dims, preferred_element_type=jnp.float32)


def line(length, dim):
    return lax.broadcasted_iota(jnp.int32, (length, 1) if dim == 0 else (1, length), dim)


def split(n, size):
    q = jnp.zeros_like(n)
    for k in range(1, 32):
        q = q + (n >= k * size).astype(jnp.int32)
    return q, n - q * size


def run_of_class(per_class, dim):
    return split(line(per_class, dim), per_class // CLASSES)


def run_of_halo(rows_per_residue, dim):
    j, i = split(line(STEPS // CLASSES, dim), HALO)
    return j, i + rows_per_residue - HALO


def positions(rows, dim):
    j, i = run_of_class(rows // CLASSES, dim)
    return jnp.concatenate([16 * i + 4 * j + c for c in range(CLASSES)], axis=dim)


def to_class_order(rows):
    return positions(rows, 0) == line(rows, 1)


def halo_rows(rows):
    per_residue = rows // WIDE_DILATION
    return [r * per_residue + per_residue - HALO for r in range(WIDE_DILATION)]


def project_kernel(
    tokens_hbm, gain_hbm, wk_hbm, wv_hbm, kv0_ref, s1_ref, s2_ref, s3_ref, normed_ref, x_ref, gain_ref, w_ref, sem
):
    rows = x_ref.shape[0]
    chunks = rows // CHUNK
    gain_load = pltpu.make_async_copy(gain_hbm, gain_ref, sem.at[chunks + 2 * GROUPS])
    gain_load.start()
    loads = [
        pltpu.make_async_copy(tokens_hbm.at[pl.ds(n * CHUNK, CHUNK)], x_ref.at[pl.ds(n * CHUNK, CHUNK)], sem.at[n])
        for n in range(chunks)
    ]
    for g in range(GROUPS):
        at = chunks + 2 * g
        loads.append(pltpu.make_async_copy(wk_hbm.at[g], w_ref.at[pl.ds(g * PAIR, HEAD_DIM)], sem.at[at]))
        loads.append(
            pltpu.make_async_copy(wv_hbm.at[g], w_ref.at[pl.ds(g * PAIR + HEAD_DIM, HEAD_DIM)], sem.at[at + 1])
        )
    for load in loads:
        load.start()
    pick = to_class_order(rows).astype(jnp.bfloat16)
    gain_load.wait()
    gain = gain_ref[...]
    for n in range(chunks):
        loads[n].wait()
        run = pl.ds(n * CHUNK, CHUNK)
        x = x_ref[run, :].astype(jnp.float32)
        mean = jnp.mean(x * x, axis=-1, keepdims=True)
        normed_ref[run, :] = (x * lax.rsqrt(mean + 1e-6) * gain).astype(jnp.bfloat16)
    for load in loads[chunks:]:
        load.wait()
    kv = dot(normed_ref[...], w_ref[...], NT).astype(jnp.bfloat16)
    kv = dot(pick, kv, NN).astype(jnp.bfloat16)
    kv0_ref[...] = kv[:, 0:PAIR]
    s1_ref[STEPS : STEPS + rows, :] = kv[:, PAIR : 2 * PAIR]
    s1_ref[STEPS + rows : STEPS + 2 * rows, :] = kv[:, 2 * PAIR : 3 * PAIR]
    s2_ref[STEPS : STEPS + rows, :] = kv[:, 2 * PAIR : 3 * PAIR]
    s3_ref[...] = kv[:, 2 * PAIR : 3 * PAIR]
    for r, lo in enumerate(halo_rows(rows)):
        s1_ref[r * HALO : (r + 1) * HALO, :] = kv[lo : lo + HALO, 0:PAIR]
        s2_ref[r * HALO : (r + 1) * HALO, :] = kv[lo : lo + HALO, PAIR : 2 * PAIR]


def query_kernel(normed_ref, wq_ref, q_ref):
    rows = normed_ref.shape[0]
    wq = wq_ref[...].reshape(GROUPS * HEAD_DIM, -1)
    q = (dot(normed_ref[...], wq, NT).astype(jnp.bfloat16) * jnp.bfloat16(0.125)).astype(jnp.bfloat16)
    q_ref[...] = dot(to_class_order(rows).astype(jnp.bfloat16), q, NN).astype(jnp.bfloat16)


def relay_kernel(r1_ref, r2_ref, s4_ref):
    rows = r1_ref.shape[0] // 2 - STEPS // 2
    s4_ref[0:rows, :] = r1_ref[STEPS + rows : STEPS + 2 * rows, :]
    for r, lo in enumerate(halo_rows(rows)):
        at = rows + r * HALO
        s4_ref[at : at + HALO, :] = r2_ref[STEPS + lo : STEPS + lo + HALO, :]


def slope_of(group, slot):
    n = jnp.full((1, 1), group * SLOTS + 1, jnp.int32) + slot
    return jnp.exp2(-8.0 * n.astype(jnp.float32) / (GROUPS * SLOTS))


def bias_of(distance, valid, slope):
    ok = valid & (distance >= 0) & (distance <= STEPS)
    return jnp.where(ok, -slope * distance.astype(jnp.float32), NEG_BIG)


def softmax_pieces(scores):
    top = jnp.max(scores, axis=-1, keepdims=True)
    e = jnp.exp(scores - top)
    total = jnp.sum(e, axis=-1, keepdims=True)
    return (e * (1.0 / total)).astype(jnp.bfloat16), top + jnp.log(total)


def wide_bias(rows, blocks, sp, slope, halo_block=None):
    per_class, per_residue = rows // CLASSES, rows // WIDE_DILATION
    jq, iq = run_of_class(per_class, 0)
    jk, ik = run_of_class(per_class, 1)
    js, at, ok = [], [], []
    for b in blocks:
        js.append(jk)
        at.append(ik - per_residue * b)
        ok.append(jnp.full_like(jk, b) <= sp)
    if halo_block is not None:
        jh, ih = run_of_halo(per_residue, 1)
        js.append(jh)
        at.append(ih - per_residue * halo_block)
        ok.append(jnp.full_like(jh, halo_block) <= sp)
    js, at = jnp.concatenate(js, axis=1), jnp.concatenate(at, axis=1)
    ok = jnp.concatenate([o.astype(jnp.int32) for o in ok], axis=1) > 0
    return bias_of(iq - at, (jq == js) & ok, slope)


def early_kernel(
    sp_ref, slot_ref, q_ref, kv0_ref, s1_ref, s3_ref, r1_ref, r2_ref, r3_ref, r4_ref, o_ref, l_ref, e_ref, top_ref,
    sum_ref,
):
    rows = kv0_ref.shape[0]
    sp, slot = sp_ref[0], slot_ref[0]
    per_class, per_residue = rows // CLASSES, rows // WIDE_DILATION
    runs = [pl.ds(c * per_class, per_class) for c in range(CLASSES)]
    jh, ih = run_of_halo(per_residue, 1)
    tail = jnp.concatenate([16 * ih + 4 * jh + c - rows for c in range(CLASSES)], axis=1)
    tk = jnp.concatenate([positions(rows, 1), tail], axis=1)
    bias = bias_of(positions(rows, 0) - tk, (tk >= 0) | (sp >= 1), slope_of(0, slot))
    keys = jnp.concatenate([kv0_ref[...], r1_ref[0:STEPS, :]], axis=0)
    p, l0 = softmax_pieces(dot(q_ref[:, 0:HEAD_DIM], keys[:, 0:HEAD_DIM], NT) + bias)
    o0 = dot(p, keys[:, HEAD_DIM:PAIR], NN)
    jq, iq = run_of_class(per_class, 0)
    jk, ik = run_of_class(per_class, 1)
    own = 4 * ik + jk
    tk = jnp.concatenate([own, own - per_class, 4 * ih + jh - 2 * per_class], axis=1)
    block = jnp.concatenate([jnp.zeros_like(own), jnp.full_like(own, 1), jnp.full_like(jh, 2)], axis=1)
    bias = bias_of(4 * iq + jq - tk, block <= sp, slope_of(1, slot))
    halo = STEPS // CLASSES
    keys = [
        jnp.concatenate(
            [
                s1_ref[pl.ds(STEPS + c * per_class, per_class), :],
                r1_ref[pl.ds(STEPS + c * per_class, per_class), :],
                r2_ref[pl.ds(c * halo, halo), :],
            ],
            axis=0,
        )
        for c in range(CLASSES)
    ]
    scores = [dot(q_ref[runs[c], HEAD_DIM : 2 * HEAD_DIM], keys[c][:, 0:HEAD_DIM], NT) + bias for c in range(CLASSES)]
    p, l1 = softmax_pieces(jnp.concatenate(scores, axis=0))
    o1 = [
        dot(p[c * per_class : (c + 1) * per_class], keys[c][:, HEAD_DIM:PAIR], NN) for c in range(CLASSES)
    ]
    top = jnp.maximum(l0, l1)
    w0, w1 = jnp.exp(l0 - top), jnp.exp(l1 - top)
    both = w0 + w1
    l_ref[...] = top + jnp.log(both)
    both = 1.0 / both
    o_ref[...] = (w0 * both) * o0 + (w1 * both) * jnp.concatenate(o1, axis=0)
    bias = wide_bias(rows, (0, 1, 2, 3, 4), sp, slope_of(2, slot))
    scores = []
    for c in range(CLASSES):
        lo = c * per_class
        keys = jnp.concatenate(
            [
                s3_ref[runs[c], 0:HEAD_DIM],
                r1_ref[pl.ds(STEPS + rows + lo, per_class), 0:HEAD_DIM],
                r2_ref[pl.ds(STEPS + lo, per_class), 0:HEAD_DIM],
                r3_ref[runs[c], 0:HEAD_DIM],
                r4_ref[runs[c], 0:HEAD_DIM],
            ],
            axis=0,
        )
        scores.append(dot(q_ref[runs[c], 2 * HEAD_DIM : 3 * HEAD_DIM], keys, NT) + bias)
    scores = jnp.concatenate(scores, axis=0)
    top = jnp.max(scores, axis=-1, keepdims=True)
    e = jnp.exp(scores - top)
    e_ref[...] = e
    top_ref[...] = top
    sum_ref[...] = jnp.sum(e, axis=-1, keepdims=True)


def late_kernel(
    sp_ref, slot_ref, q_ref, s3_ref, r1_ref, r2_ref, r3_ref, r4_ref, far_ref, o_ref, l_ref, e_ref, top_ref, sum_ref,
    mix_ref, lw_ref,
):
    rows = s3_ref.shape[0]
    sp, slot = sp_ref[0], slot_ref[0]
    per_class = rows // CLASSES
    halo = STEPS // CLASSES
    runs = [pl.ds(c * per_class, per_class) for c in range(CLASSES)]
    bias = wide_bias(rows, (5,), sp, slope_of(2, slot), halo_block=6)
    keys = [
        jnp.concatenate(
            [far_ref[runs[c], :], far_ref[pl.ds(rows + c * halo, halo), :]],
            axis=0,
        )
        for c in range(CLASSES)
    ]
    scores = jnp.concatenate(
        [dot(q_ref[runs[c], 2 * HEAD_DIM : 3 * HEAD_DIM], keys[c][:, 0:HEAD_DIM], NT) + bias for c in range(CLASSES)], axis=0
    )
    top0 = top_ref[...]
    top = jnp.maximum(top0, jnp.max(scores, axis=-1, keepdims=True))
    e = jnp.exp(scores - top)
    shrink = jnp.exp(top0 - top)
    total = sum_ref[...] * shrink + jnp.sum(e, axis=-1, keepdims=True)
    scale = 1.0 / total
    l2 = top + jnp.log(total)
    p = (e * scale).astype(jnp.bfloat16)
    p_early = (e_ref[...] * (shrink * scale)).astype(jnp.bfloat16)
    out = []
    for c in range(CLASSES):
        lo = c * per_class
        early = jnp.concatenate(
            [
                s3_ref[runs[c], HEAD_DIM:PAIR],
                r1_ref[pl.ds(STEPS + rows + lo, per_class), HEAD_DIM:PAIR],
                r2_ref[pl.ds(STEPS + lo, per_class), HEAD_DIM:PAIR],
                r3_ref[runs[c], HEAD_DIM:PAIR],
                r4_ref[runs[c], HEAD_DIM:PAIR],
            ],
            axis=0,
        )
        out.append(
            dot(p_early[lo : lo + per_class], early, NN) + dot(p[lo : lo + per_class], keys[c][:, HEAD_DIM:PAIR], NN)
        )
    l01 = l_ref[...]
    top = jnp.maximum(l01, l2)
    w01, w2 = jnp.exp(l01 - top), jnp.exp(l2 - top)
    both = w01 + w2
    lw = top + jnp.log(both)
    both = 1.0 / both
    mixed = ((w01 * both) * o_ref[...] + (w2 * both) * jnp.concatenate(out, axis=0)).astype(jnp.bfloat16)
    pick = to_class_order(rows)
    mix = dot(mixed, pick.astype(jnp.bfloat16), TN).astype(jnp.bfloat16)
    for n in range(mix_ref.shape[0]):
        mix_ref[n] = mix
    lw_ref[...] = jnp.sum(jnp.where(pick, lw, 0.0), axis=0, keepdims=True)


def output_kernel(mix_ref, w_ref, out_ref):
    mixed = mix_ref[...].reshape(-1, out_ref.shape[0])
    out_ref[...] = dot(mixed, w_ref[...], TN).astype(jnp.bfloat16)


VMEM = pl.BlockSpec(memory_space=pltpu.VMEM)
SMEM = pl.BlockSpec(memory_space=pltpu.SMEM)
HBM = pl.BlockSpec(memory_space=pltpu.HBM)


def call(body, operands, outs, specs=None, scratch=()):
    return pl.pallas_call(
        body,
        in_specs=specs or [VMEM] * len(operands),
        out_specs=[VMEM] * len(outs),
        out_shape=[jax.ShapeDtypeStruct(s, d) for s, d in outs],
        scratch_shapes=list(scratch),
        compiler_params=pltpu.CompilerParams(vmem_limit_bytes=20 * 2**20),
    )(*operands)


def in_hbm(value):
    return pltpu.with_memory_space_constraint(value, pltpu.HBM)


def from_behind(value, by):
    devices = lax.axis_size("sp")
    return lax.ppermute(value, "sp", [(i, i + by) for i in range(devices - by)])


def layer(tokens, norm_gain, w_query, w_key, w_value, w_out):
    rows, width = tokens.shape
    bf16, f32 = jnp.bfloat16, jnp.float32
    sp = lax.axis_index("sp").reshape(1)
    slot = lax.axis_index("tp").reshape(1)
    kv0, s1, s2, s3, normed = call(
        project_kernel,
        (in_hbm(tokens), in_hbm(norm_gain.reshape(1, -1)), in_hbm(w_key), in_hbm(w_value)),
        [
            ((rows, PAIR), bf16),
            ((STEPS + 2 * rows, PAIR), bf16),
            ((STEPS + rows, PAIR), bf16),
            ((rows, PAIR), bf16),
            ((rows, width), bf16),
        ],
        specs=[HBM] * 4,
        scratch=[
            pltpu.VMEM((rows, width), bf16),
            pltpu.VMEM((1, width), f32),
            pltpu.VMEM((GROUPS * PAIR, width), bf16),
            pltpu.SemaphoreType.DMA((rows // CHUNK + 2 * GROUPS + 1,)),
        ],
    )
    r1 = from_behind(s1, 1)
    r2 = from_behind(s2, 2)
    r3 = from_behind(s3, 3)
    r4 = from_behind(s3, 4)
    (q,) = call(query_kernel, (normed, w_query), [((rows, GROUPS * HEAD_DIM), bf16)])
    (s4,) = call(relay_kernel, (r1, r2), [((STEPS + rows, PAIR), bf16)])
    far = from_behind(s4, 4)
    o, l, e, top, total = call(
        early_kernel,
        (sp, slot, q, kv0, s1, s3, r1, r2, r3, r4),
        [((rows, HEAD_DIM), f32), ((rows, 1), f32), ((rows, 5 * rows // CLASSES), f32), ((rows, 1), f32), ((rows, 1), f32)],
        specs=[SMEM] * 2 + [VMEM] * 8,
    )
    devices = lax.axis_size("tp")
    mix, log_weight = call(
        late_kernel,
        (sp, slot, q, s3, r1, r2, r3, r4, far, o, l, e, top, total),
        [((devices, HEAD_DIM, rows), bf16), ((1, rows), f32)],
        specs=[SMEM] * 2 + [VMEM] * 12,
    )
    everyone = lax.all_to_all(mix, "tp", 0, 0, tiled=True)
    (projected,) = call(output_kernel, (everyone, w_out), [((rows, w_out.shape[1]), bf16)])
    return projected, log_weight


def solution(mesh):
    in_specs = (P("sp", None), P(), P(None, "tp", None), P(None, "tp", None), P(None, "tp", None), P(None, "tp"))
    out_specs = (P("sp", "tp"), P("tp", "sp"))
    return jax.shard_map(layer, mesh=mesh, in_specs=in_specs, out_specs=out_specs, check_vma=False)
```

```python
import jax
import jax.numpy as jnp
from jax import lax
from jax.experimental import pallas as pl
from jax.experimental.pallas import tpu as pltpu
from jax.sharding import PartitionSpec as P


HEAD_DIM = 64
SLOTS = 8
STEPS = 128
GROUPS = 3
WIDE_DILATION = 16
NEG_BIG = -1e30

CLASSES = 4
PAIR = 2 * HEAD_DIM
CHUNK = 128
HALO = STEPS // WIDE_DILATION
NT = (((1,), (1,)), ((), ()))
NN = (((1,), (0,)), ((), ()))
TN = (((0,), (0,)), ((), ()))


def dot(a, b, dims):
    return lax.dot_general(a, b, dims, preferred_element_type=jnp.float32)


def line(length, dim):
    return lax.broadcasted_iota(jnp.int32, (length, 1) if dim == 0 else (1, length), dim)


def split(n, size):
    q = jnp.zeros_like(n)
    for k in range(1, 32):
        q = q + (n >= k * size).astype(jnp.int32)
    return q, n - q * size


def run_of_class(per_class, dim):
    return split(line(per_class, dim), per_class // CLASSES)


def run_of_halo(rows_per_residue, dim):
    j, i = split(line(STEPS // CLASSES, dim), HALO)
    return j, i + rows_per_residue - HALO


def positions(rows, dim):
    j, i = run_of_class(rows // CLASSES, dim)
    return jnp.concatenate([16 * i + 4 * j + c for c in range(CLASSES)], axis=dim)


def to_class_order(rows):
    return positions(rows, 0) == line(rows, 1)


def halo_rows(rows):
    per_residue = rows // WIDE_DILATION
    return [r * per_residue + per_residue - HALO for r in range(WIDE_DILATION)]


def project_kernel(
    tokens_hbm, gain_hbm, wk_hbm, wv_hbm, kv0_ref, s1_ref, s2_ref, s3_ref, normed_ref, x_ref, gain_ref, w_ref, sem
):
    rows = x_ref.shape[0]
    chunks = rows // CHUNK
    gain_load = pltpu.make_async_copy(gain_hbm, gain_ref, sem.at[chunks + 2 * GROUPS])
    gain_load.start()
    loads = [
        pltpu.make_async_copy(tokens_hbm.at[pl.ds(n * CHUNK, CHUNK)], x_ref.at[pl.ds(n * CHUNK, CHUNK)], sem.at[n])
        for n in range(chunks)
    ]
    for g in range(GROUPS):
        at = chunks + 2 * g
        loads.append(pltpu.make_async_copy(wk_hbm.at[g], w_ref.at[pl.ds(g * PAIR, HEAD_DIM)], sem.at[at]))
        loads.append(
            pltpu.make_async_copy(wv_hbm.at[g], w_ref.at[pl.ds(g * PAIR + HEAD_DIM, HEAD_DIM)], sem.at[at + 1])
        )
    for load in loads:
        load.start()
    pick = to_class_order(rows).astype(jnp.bfloat16)
    gain_load.wait()
    gain = gain_ref[...]
    for n in range(chunks):
        loads[n].wait()
        run = pl.ds(n * CHUNK, CHUNK)
        x = x_ref[run, :].astype(jnp.float32)
        mean = jnp.mean(x * x, axis=-1, keepdims=True)
        normed_ref[run, :] = (x * lax.rsqrt(mean + 1e-6) * gain).astype(jnp.bfloat16)
    for load in loads[chunks:]:
        load.wait()
    kv = dot(normed_ref[...], w_ref[...], NT).astype(jnp.bfloat16)
    kv = dot(pick, kv, NN).astype(jnp.bfloat16)
    kv0_ref[...] = kv[:, 0:PAIR]
    s1_ref[STEPS : STEPS + rows, :] = kv[:, PAIR : 2 * PAIR]
    s1_ref[STEPS + rows : STEPS + 2 * rows, :] = kv[:, 2 * PAIR : 3 * PAIR]
    s2_ref[STEPS : STEPS + rows, :] = kv[:, 2 * PAIR : 3 * PAIR]
    s3_ref[...] = kv[:, 2 * PAIR : 3 * PAIR]
    for r, lo in enumerate(halo_rows(rows)):
        s1_ref[r * HALO : (r + 1) * HALO, :] = kv[lo : lo + HALO, 0:PAIR]
        s2_ref[r * HALO : (r + 1) * HALO, :] = kv[lo : lo + HALO, PAIR : 2 * PAIR]


def query_kernel(normed_ref, wq_ref, q_ref):
    rows = normed_ref.shape[0]
    wq = wq_ref[...].reshape(GROUPS * HEAD_DIM, -1)
    q = (dot(normed_ref[...], wq, NT).astype(jnp.bfloat16) * jnp.bfloat16(0.125)).astype(jnp.bfloat16)
    q_ref[...] = dot(to_class_order(rows).astype(jnp.bfloat16), q, NN).astype(jnp.bfloat16)


def relay_kernel(s3_ref, r1_ref, s4_ref):
    rows = s3_ref.shape[0]
    s4_ref[0:rows, :] = s3_ref[...]
    s4_ref[rows : 2 * rows, :] = r1_ref[STEPS + rows : STEPS + 2 * rows, :]


def relay_tail_kernel(r2_ref, s6_ref):
    for r, lo in enumerate(halo_rows(r2_ref.shape[0] - STEPS)):
        s6_ref[r * HALO : (r + 1) * HALO, :] = r2_ref[STEPS + lo : STEPS + lo + HALO, :]


def slope_of(group, slot):
    n = jnp.full((1, 1), group * SLOTS + 1, jnp.int32) + slot
    return jnp.exp2(-8.0 * n.astype(jnp.float32) / (GROUPS * SLOTS))


def bias_of(distance, valid, slope):
    ok = valid & (distance >= 0) & (distance <= STEPS)
    return jnp.where(ok, -slope * distance.astype(jnp.float32), NEG_BIG)


def softmax_pieces(scores):
    top = jnp.max(scores, axis=-1, keepdims=True)
    e = jnp.exp(scores - top)
    total = jnp.sum(e, axis=-1, keepdims=True)
    return (e * (1.0 / total)).astype(jnp.bfloat16), top + jnp.log(total)


def wide_bias(rows, blocks, sp, slope, halo_block=None):
    per_class, per_residue = rows // CLASSES, rows // WIDE_DILATION
    jq, iq = run_of_class(per_class, 0)
    jk, ik = run_of_class(per_class, 1)
    js, at, ok = [], [], []
    for b in blocks:
        js.append(jk)
        at.append(ik - per_residue * b)
        ok.append(jnp.full_like(jk, b) <= sp)
    if halo_block is not None:
        jh, ih = run_of_halo(per_residue, 1)
        js.append(jh)
        at.append(ih - per_residue * halo_block)
        ok.append(jnp.full_like(jh, halo_block) <= sp)
    js, at = jnp.concatenate(js, axis=1), jnp.concatenate(at, axis=1)
    ok = jnp.concatenate([o.astype(jnp.int32) for o in ok], axis=1) > 0
    return bias_of(iq - at, (jq == js) & ok, slope)


def early_kernel(
    sp_ref, slot_ref, q_ref, kv0_ref, s1_ref, s3_ref, r1_ref, r2_ref, r3_ref, o_ref, l_ref, e_ref, top_ref, sum_ref
):
    rows = kv0_ref.shape[0]
    sp, slot = sp_ref[0], slot_ref[0]
    per_class, per_residue = rows // CLASSES, rows // WIDE_DILATION
    runs = [pl.ds(c * per_class, per_class) for c in range(CLASSES)]
    jh, ih = run_of_halo(per_residue, 1)
    tail = jnp.concatenate([16 * ih + 4 * jh + c - rows for c in range(CLASSES)], axis=1)
    tk = jnp.concatenate([positions(rows, 1), tail], axis=1)
    bias = bias_of(positions(rows, 0) - tk, (tk >= 0) | (sp >= 1), slope_of(0, slot))
    keys = jnp.concatenate([kv0_ref[...], r1_ref[0:STEPS, :]], axis=0)
    p, l0 = softmax_pieces(dot(q_ref[:, 0:HEAD_DIM], keys[:, 0:HEAD_DIM], NT) + bias)
    o0 = dot(p, keys[:, HEAD_DIM:PAIR], NN)
    jq, iq = run_of_class(per_class, 0)
    jk, ik = run_of_class(per_class, 1)
    own = 4 * ik + jk
    tk = jnp.concatenate([own, own - per_class, 4 * ih + jh - 2 * per_class], axis=1)
    block = jnp.concatenate([jnp.zeros_like(own), jnp.full_like(own, 1), jnp.full_like(jh, 2)], axis=1)
    bias = bias_of(4 * iq + jq - tk, block <= sp, slope_of(1, slot))
    halo = STEPS // CLASSES
    keys = [
        jnp.concatenate(
            [
                s1_ref[pl.ds(STEPS + c * per_class, per_class), :],
                r1_ref[pl.ds(STEPS + c * per_class, per_class), :],
                r2_ref[pl.ds(c * halo, halo), :],
            ],
            axis=0,
        )
        for c in range(CLASSES)
    ]
    scores = [dot(q_ref[runs[c], HEAD_DIM : 2 * HEAD_DIM], keys[c][:, 0:HEAD_DIM], NT) + bias for c in range(CLASSES)]
    p, l1 = softmax_pieces(jnp.concatenate(scores, axis=0))
    o1 = [
        dot(p[c * per_class : (c + 1) * per_class], keys[c][:, HEAD_DIM:PAIR], NN) for c in range(CLASSES)
    ]
    top = jnp.maximum(l0, l1)
    w0, w1 = jnp.exp(l0 - top), jnp.exp(l1 - top)
    both = w0 + w1
    l_ref[...] = top + jnp.log(both)
    both = 1.0 / both
    o_ref[...] = (w0 * both) * o0 + (w1 * both) * jnp.concatenate(o1, axis=0)
    bias = wide_bias(rows, (0, 1, 2, 3), sp, slope_of(2, slot))
    scores = []
    for c in range(CLASSES):
        lo = c * per_class
        keys = jnp.concatenate(
            [
                s3_ref[runs[c], 0:HEAD_DIM],
                r1_ref[pl.ds(STEPS + rows + lo, per_class), 0:HEAD_DIM],
                r2_ref[pl.ds(STEPS + lo, per_class), 0:HEAD_DIM],
                r3_ref[runs[c], 0:HEAD_DIM],
            ],
            axis=0,
        )
        scores.append(dot(q_ref[runs[c], 2 * HEAD_DIM : 3 * HEAD_DIM], keys, NT) + bias)
    scores = jnp.concatenate(scores, axis=0)
    top = jnp.max(scores, axis=-1, keepdims=True)
    e = jnp.exp(scores - top)
    e_ref[...] = e
    top_ref[...] = top
    sum_ref[...] = jnp.sum(e, axis=-1, keepdims=True)


def late_kernel(
    sp_ref, slot_ref, q_ref, s3_ref, r1_ref, r2_ref, r3_ref, r4_ref, r6_ref, o_ref, l_ref, e_ref, top_ref, sum_ref,
    mix_ref, lw_ref,
):
    rows = s3_ref.shape[0]
    sp, slot = sp_ref[0], slot_ref[0]
    per_class = rows // CLASSES
    halo = STEPS // CLASSES
    runs = [pl.ds(c * per_class, per_class) for c in range(CLASSES)]
    bias = wide_bias(rows, (4, 5), sp, slope_of(2, slot), halo_block=6)
    keys = [
        jnp.concatenate(
            [r4_ref[runs[c], :], r4_ref[pl.ds(rows + c * per_class, per_class), :], r6_ref[pl.ds(c * halo, halo), :]],
            axis=0,
        )
        for c in range(CLASSES)
    ]
    scores = jnp.concatenate(
        [dot(q_ref[runs[c], 2 * HEAD_DIM : 3 * HEAD_DIM], keys[c][:, 0:HEAD_DIM], NT) + bias for c in range(CLASSES)], axis=0
    )
    top0 = top_ref[...]
    top = jnp.maximum(top0, jnp.max(scores, axis=-1, keepdims=True))
    e = jnp.exp(scores - top)
    shrink = jnp.exp(top0 - top)
    total = sum_ref[...] * shrink + jnp.sum(e, axis=-1, keepdims=True)
    scale = 1.0 / total
    l2 = top + jnp.log(total)
    p = (e * scale).astype(jnp.bfloat16)
    p_early = (e_ref[...] * (shrink * scale)).astype(jnp.bfloat16)
    out = []
    for c in range(CLASSES):
        lo = c * per_class
        early = jnp.concatenate(
            [
                s3_ref[runs[c], HEAD_DIM:PAIR],
                r1_ref[pl.ds(STEPS + rows + lo, per_class), HEAD_DIM:PAIR],
                r2_ref[pl.ds(STEPS + lo, per_class), HEAD_DIM:PAIR],
                r3_ref[runs[c], HEAD_DIM:PAIR],
            ],
            axis=0,
        )
        out.append(
            dot(p_early[lo : lo + per_class], early, NN) + dot(p[lo : lo + per_class], keys[c][:, HEAD_DIM:PAIR], NN)
        )
    l01 = l_ref[...]
    top = jnp.maximum(l01, l2)
    w01, w2 = jnp.exp(l01 - top), jnp.exp(l2 - top)
    both = w01 + w2
    lw = top + jnp.log(both)
    both = 1.0 / both
    mixed = ((w01 * both) * o_ref[...] + (w2 * both) * jnp.concatenate(out, axis=0)).astype(jnp.bfloat16)
    pick = to_class_order(rows)
    mix = dot(mixed, pick.astype(jnp.bfloat16), TN).astype(jnp.bfloat16)
    for n in range(mix_ref.shape[0]):
        mix_ref[n] = mix
    lw_ref[...] = jnp.sum(jnp.where(pick, lw, 0.0), axis=0, keepdims=True)


def output_kernel(mix_ref, w_ref, out_ref):
    mixed = mix_ref[...].reshape(-1, out_ref.shape[0])
    out_ref[...] = dot(mixed, w_ref[...], TN).astype(jnp.bfloat16)


VMEM = pl.BlockSpec(memory_space=pltpu.VMEM)
SMEM = pl.BlockSpec(memory_space=pltpu.SMEM)
HBM = pl.BlockSpec(memory_space=pltpu.HBM)


def call(body, operands, outs, specs=None, scratch=()):
    return pl.pallas_call(
        body,
        in_specs=specs or [VMEM] * len(operands),
        out_specs=[VMEM] * len(outs),
        out_shape=[jax.ShapeDtypeStruct(s, d) for s, d in outs],
        scratch_shapes=list(scratch),
        compiler_params=pltpu.CompilerParams(vmem_limit_bytes=20 * 2**20),
    )(*operands)


def in_hbm(value):
    return pltpu.with_memory_space_constraint(value, pltpu.HBM)


def from_behind(value, by):
    devices = lax.axis_size("sp")
    return lax.ppermute(value, "sp", [(i, i + by) for i in range(devices - by)])


def layer(tokens, norm_gain, w_query, w_key, w_value, w_out):
    rows, width = tokens.shape
    bf16, f32 = jnp.bfloat16, jnp.float32
    sp = lax.axis_index("sp").reshape(1)
    slot = lax.axis_index("tp").reshape(1)
    kv0, s1, s2, s3, normed = call(
        project_kernel,
        (in_hbm(tokens), in_hbm(norm_gain.reshape(1, -1)), in_hbm(w_key), in_hbm(w_value)),
        [
            ((rows, PAIR), bf16),
            ((STEPS + 2 * rows, PAIR), bf16),
            ((STEPS + rows, PAIR), bf16),
            ((rows, PAIR), bf16),
            ((rows, width), bf16),
        ],
        specs=[HBM] * 4,
        scratch=[
            pltpu.VMEM((rows, width), bf16),
            pltpu.VMEM((1, width), f32),
            pltpu.VMEM((GROUPS * PAIR, width), bf16),
            pltpu.SemaphoreType.DMA((rows // CHUNK + 2 * GROUPS + 1,)),
        ],
    )
    r1 = from_behind(s1, 1)
    r2 = from_behind(s2, 2)
    r3 = from_behind(s3, 3)
    (s4,) = call(relay_kernel, (s3, r1), [((2 * rows, PAIR), bf16)])
    r4 = from_behind(s4, 4)
    (q,) = call(query_kernel, (normed, w_query), [((rows, GROUPS * HEAD_DIM), bf16)])
    (s6,) = call(relay_tail_kernel, (r2,), [((STEPS, PAIR), bf16)])
    r6 = from_behind(s6, 4)
    o, l, e, top, total = call(
        early_kernel,
        (sp, slot, q, kv0, s1, s3, r1, r2, r3),
        [((rows, HEAD_DIM), f32), ((rows, 1), f32), ((rows, rows), f32), ((rows, 1), f32), ((rows, 1), f32)],
        specs=[SMEM] * 2 + [VMEM] * 7,
    )
    devices = lax.axis_size("tp")
    mix, log_weight = call(
        late_kernel,
        (sp, slot, q, s3, r1, r2, r3, r4, r6, o, l, e, top, total),
        [((devices, HEAD_DIM, rows), bf16), ((1, rows), f32)],
        specs=[SMEM] * 2 + [VMEM] * 12,
    )
    everyone = lax.all_to_all(mix, "tp", 0, 0, tiled=True)
    (projected,) = call(output_kernel, (everyone, w_out), [((rows, w_out.shape[1]), bf16)])
    return projected, log_weight


def solution(mesh):
    in_specs = (P("sp", None), P(), P(None, "tp", None), P(None, "tp", None), P(None, "tp", None), P(None, "tp"))
    out_specs = (P("sp", "tp"), P("tp", "sp"))
    return jax.shard_map(layer, mesh=mesh, in_specs=in_specs, out_specs=out_specs, check_vma=False)
```

```python
import jax
import jax.numpy as jnp
from jax import lax
from jax.experimental import pallas as pl
from jax.experimental.pallas import tpu as pltpu
from jax.sharding import PartitionSpec as P


HEAD_DIM = 64
SLOTS = 8
STEPS = 128
GROUPS = 3
WIDE_DILATION = 16
NEG_BIG = -1e30

CLASSES = 4
PAIR = 2 * HEAD_DIM
CHUNK = 128
HALO = STEPS // WIDE_DILATION
NT = (((1,), (1,)), ((), ()))
NN = (((1,), (0,)), ((), ()))
TN = (((0,), (0,)), ((), ()))


def dot(a, b, dims):
    return lax.dot_general(a, b, dims, preferred_element_type=jnp.float32)


def line(length, dim):
    return lax.broadcasted_iota(jnp.int32, (length, 1) if dim == 0 else (1, length), dim)


def split(n, size):
    q = jnp.zeros_like(n)
    for k in range(1, 32):
        q = q + (n >= k * size).astype(jnp.int32)
    return q, n - q * size


def run_of_class(per_class, dim):
    return split(line(per_class, dim), per_class // CLASSES)


def run_of_halo(rows_per_residue, dim):
    j, i = split(line(STEPS // CLASSES, dim), HALO)
    return j, i + rows_per_residue - HALO


def positions(rows, dim):
    j, i = run_of_class(rows // CLASSES, dim)
    return jnp.concatenate([16 * i + 4 * j + c for c in range(CLASSES)], axis=dim)


def to_class_order(rows):
    return positions(rows, 0) == line(rows, 1)


def halo_rows(rows):
    per_residue = rows // WIDE_DILATION
    return [r * per_residue + per_residue - HALO for r in range(WIDE_DILATION)]


def project_kernel(
    tokens_hbm, gain_hbm, wk_hbm, wv_hbm, kv0_ref, s1_ref, s2_ref, s3_ref, normed_ref, x_ref, gain_ref, w_ref, sem
):
    rows = x_ref.shape[0]
    chunks = rows // CHUNK
    gain_load = pltpu.make_async_copy(gain_hbm, gain_ref, sem.at[chunks + 2 * GROUPS])
    gain_load.start()
    loads = [
        pltpu.make_async_copy(tokens_hbm.at[pl.ds(n * CHUNK, CHUNK)], x_ref.at[pl.ds(n * CHUNK, CHUNK)], sem.at[n])
        for n in range(chunks)
    ]
    for g in range(GROUPS):
        at = chunks + 2 * g
        loads.append(pltpu.make_async_copy(wk_hbm.at[g], w_ref.at[pl.ds(g * PAIR, HEAD_DIM)], sem.at[at]))
        loads.append(
            pltpu.make_async_copy(wv_hbm.at[g], w_ref.at[pl.ds(g * PAIR + HEAD_DIM, HEAD_DIM)], sem.at[at + 1])
        )
    for load in loads:
        load.start()
    pick = to_class_order(rows).astype(jnp.bfloat16)
    gain_load.wait()
    gain = gain_ref[...]
    for n in range(chunks):
        loads[n].wait()
        run = pl.ds(n * CHUNK, CHUNK)
        x = x_ref[run, :].astype(jnp.float32)
        mean = jnp.mean(x * x, axis=-1, keepdims=True)
        normed_ref[run, :] = (x * lax.rsqrt(mean + 1e-6) * gain).astype(jnp.bfloat16)
    for load in loads[chunks:]:
        load.wait()
    kv = dot(normed_ref[...], w_ref[...], NT).astype(jnp.bfloat16)
    kv = dot(pick, kv, NN).astype(jnp.bfloat16)
    kv0_ref[...] = kv[:, 0:PAIR]
    s1_ref[STEPS : STEPS + rows, :] = kv[:, PAIR : 2 * PAIR]
    s1_ref[STEPS + rows : STEPS + 2 * rows, :] = kv[:, 2 * PAIR : 3 * PAIR]
    s2_ref[STEPS : STEPS + rows, :] = kv[:, 2 * PAIR : 3 * PAIR]
    s3_ref[...] = kv[:, 2 * PAIR : 3 * PAIR]
    for r, lo in enumerate(halo_rows(rows)):
        s1_ref[r * HALO : (r + 1) * HALO, :] = kv[lo : lo + HALO, 0:PAIR]
        s2_ref[r * HALO : (r + 1) * HALO, :] = kv[lo : lo + HALO, PAIR : 2 * PAIR]


def query_kernel(normed_ref, wq_ref, q_ref):
    rows = normed_ref.shape[0]
    wq = wq_ref[...].reshape(GROUPS * HEAD_DIM, -1)
    q = (dot(normed_ref[...], wq, NT).astype(jnp.bfloat16) * jnp.bfloat16(0.125)).astype(jnp.bfloat16)
    q_ref[...] = dot(to_class_order(rows).astype(jnp.bfloat16), q, NN).astype(jnp.bfloat16)


def relay_kernel(s3_ref, r1_ref, r2_ref, s4_ref):
    rows = s3_ref.shape[0]
    s4_ref[0:rows, :] = s3_ref[...]
    s4_ref[rows : 2 * rows, :] = r1_ref[STEPS + rows : STEPS + 2 * rows, :]
    for r, lo in enumerate(halo_rows(rows)):
        at = 2 * rows + r * HALO
        s4_ref[at : at + HALO, :] = r2_ref[STEPS + lo : STEPS + lo + HALO, :]


def slope_of(group, slot):
    n = jnp.full((1, 1), group * SLOTS + 1, jnp.int32) + slot
    return jnp.exp2(-8.0 * n.astype(jnp.float32) / (GROUPS * SLOTS))


def bias_of(distance, valid, slope):
    ok = valid & (distance >= 0) & (distance <= STEPS)
    return jnp.where(ok, -slope * distance.astype(jnp.float32), NEG_BIG)


def softmax_pieces(scores):
    top = jnp.max(scores, axis=-1, keepdims=True)
    e = jnp.exp(scores - top)
    total = jnp.sum(e, axis=-1, keepdims=True)
    return (e * (1.0 / total)).astype(jnp.bfloat16), top + jnp.log(total)


def wide_bias(rows, blocks, sp, slope, halo_block=None):
    per_class, per_residue = rows // CLASSES, rows // WIDE_DILATION
    jq, iq = run_of_class(per_class, 0)
    jk, ik = run_of_class(per_class, 1)
    js, at, ok = [], [], []
    for b in blocks:
        js.append(jk)
        at.append(ik - per_residue * b)
        ok.append(jnp.full_like(jk, b) <= sp)
    if halo_block is not None:
        jh, ih = run_of_halo(per_residue, 1)
        js.append(jh)
        at.append(ih - per_residue * halo_block)
        ok.append(jnp.full_like(jh, halo_block) <= sp)
    js, at = jnp.concatenate(js, axis=1), jnp.concatenate(at, axis=1)
    ok = jnp.concatenate([o.astype(jnp.int32) for o in ok], axis=1) > 0
    return bias_of(iq - at, (jq == js) & ok, slope)


def early_kernel(
    sp_ref, slot_ref, q_ref, kv0_ref, s1_ref, s3_ref, r1_ref, r2_ref, r3_ref, o_ref, l_ref, e_ref, top_ref, sum_ref
):
    rows = kv0_ref.shape[0]
    sp, slot = sp_ref[0], slot_ref[0]
    per_class, per_residue = rows // CLASSES, rows // WIDE_DILATION
    runs = [pl.ds(c * per_class, per_class) for c in range(CLASSES)]
    jh, ih = run_of_halo(per_residue, 1)
    tail = jnp.concatenate([16 * ih + 4 * jh + c - rows for c in range(CLASSES)], axis=1)
    tk = jnp.concatenate([positions(rows, 1), tail], axis=1)
    bias = bias_of(positions(rows, 0) - tk, (tk >= 0) | (sp >= 1), slope_of(0, slot))
    keys = jnp.concatenate([kv0_ref[...], r1_ref[0:STEPS, :]], axis=0)
    p, l0 = softmax_pieces(dot(q_ref[:, 0:HEAD_DIM], keys[:, 0:HEAD_DIM], NT) + bias)
    o0 = dot(p, keys[:, HEAD_DIM:PAIR], NN)
    jq, iq = run_of_class(per_class, 0)
    jk, ik = run_of_class(per_class, 1)
    own = 4 * ik + jk
    tk = jnp.concatenate([own, own - per_class, 4 * ih + jh - 2 * per_class], axis=1)
    block = jnp.concatenate([jnp.zeros_like(own), jnp.full_like(own, 1), jnp.full_like(jh, 2)], axis=1)
    bias = bias_of(4 * iq + jq - tk, block <= sp, slope_of(1, slot))
    halo = STEPS // CLASSES
    keys = [
        jnp.concatenate(
            [
                s1_ref[pl.ds(STEPS + c * per_class, per_class), :],
                r1_ref[pl.ds(STEPS + c * per_class, per_class), :],
                r2_ref[pl.ds(c * halo, halo), :],
            ],
            axis=0,
        )
        for c in range(CLASSES)
    ]
    scores = [dot(q_ref[runs[c], HEAD_DIM : 2 * HEAD_DIM], keys[c][:, 0:HEAD_DIM], NT) + bias for c in range(CLASSES)]
    p, l1 = softmax_pieces(jnp.concatenate(scores, axis=0))
    o1 = [
        dot(p[c * per_class : (c + 1) * per_class], keys[c][:, HEAD_DIM:PAIR], NN) for c in range(CLASSES)
    ]
    top = jnp.maximum(l0, l1)
    w0, w1 = jnp.exp(l0 - top), jnp.exp(l1 - top)
    both = w0 + w1
    l_ref[...] = top + jnp.log(both)
    both = 1.0 / both
    o_ref[...] = (w0 * both) * o0 + (w1 * both) * jnp.concatenate(o1, axis=0)
    bias = wide_bias(rows, (0, 1, 2, 3), sp, slope_of(2, slot))
    scores = []
    for c in range(CLASSES):
        lo = c * per_class
        keys = jnp.concatenate(
            [
                s3_ref[runs[c], 0:HEAD_DIM],
                r1_ref[pl.ds(STEPS + rows + lo, per_class), 0:HEAD_DIM],
                r2_ref[pl.ds(STEPS + lo, per_class), 0:HEAD_DIM],
                r3_ref[runs[c], 0:HEAD_DIM],
            ],
            axis=0,
        )
        scores.append(dot(q_ref[runs[c], 2 * HEAD_DIM : 3 * HEAD_DIM], keys, NT) + bias)
    scores = jnp.concatenate(scores, axis=0)
    top = jnp.max(scores, axis=-1, keepdims=True)
    e = jnp.exp(scores - top)
    e_ref[...] = e
    top_ref[...] = top
    sum_ref[...] = jnp.sum(e, axis=-1, keepdims=True)


def late_kernel(
    sp_ref, slot_ref, q_ref, s3_ref, r1_ref, r2_ref, r3_ref, r4_ref, o_ref, l_ref, e_ref, top_ref, sum_ref, mix_ref, lw_ref
):
    rows = s3_ref.shape[0]
    sp, slot = sp_ref[0], slot_ref[0]
    per_class = rows // CLASSES
    halo = STEPS // CLASSES
    runs = [pl.ds(c * per_class, per_class) for c in range(CLASSES)]
    bias = wide_bias(rows, (4, 5), sp, slope_of(2, slot), halo_block=6)
    keys = [
        jnp.concatenate(
            [r4_ref[runs[c], :], r4_ref[pl.ds(rows + c * per_class, per_class), :], r4_ref[pl.ds(2 * rows + c * halo, halo), :]],
            axis=0,
        )
        for c in range(CLASSES)
    ]
    scores = jnp.concatenate(
        [dot(q_ref[runs[c], 2 * HEAD_DIM : 3 * HEAD_DIM], keys[c][:, 0:HEAD_DIM], NT) + bias for c in range(CLASSES)], axis=0
    )
    top0 = top_ref[...]
    top = jnp.maximum(top0, jnp.max(scores, axis=-1, keepdims=True))
    e = jnp.exp(scores - top)
    shrink = jnp.exp(top0 - top)
    total = sum_ref[...] * shrink + jnp.sum(e, axis=-1, keepdims=True)
    scale = 1.0 / total
    l2 = top + jnp.log(total)
    p = (e * scale).astype(jnp.bfloat16)
    p_early = (e_ref[...] * (shrink * scale)).astype(jnp.bfloat16)
    out = []
    for c in range(CLASSES):
        lo = c * per_class
        early = jnp.concatenate(
            [
                s3_ref[runs[c], HEAD_DIM:PAIR],
                r1_ref[pl.ds(STEPS + rows + lo, per_class), HEAD_DIM:PAIR],
                r2_ref[pl.ds(STEPS + lo, per_class), HEAD_DIM:PAIR],
                r3_ref[runs[c], HEAD_DIM:PAIR],
            ],
            axis=0,
        )
        out.append(
            dot(p_early[lo : lo + per_class], early, NN) + dot(p[lo : lo + per_class], keys[c][:, HEAD_DIM:PAIR], NN)
        )
    l01 = l_ref[...]
    top = jnp.maximum(l01, l2)
    w01, w2 = jnp.exp(l01 - top), jnp.exp(l2 - top)
    both = w01 + w2
    lw_ref[...] = top + jnp.log(both)
    both = 1.0 / both
    mixed = ((w01 * both) * o_ref[...] + (w2 * both) * jnp.concatenate(out, axis=0)).astype(jnp.bfloat16)
    mix = dot(mixed, to_class_order(rows).astype(jnp.bfloat16), TN).astype(jnp.bfloat16)
    for n in range(mix_ref.shape[0]):
        mix_ref[n] = mix


def log_weight_kernel(lw_ref, out_ref):
    out_ref[...] = jnp.sum(jnp.where(to_class_order(lw_ref.shape[0]), lw_ref[...], 0.0), axis=0, keepdims=True)


def output_kernel(mix_ref, w_ref, out_ref):
    mixed = mix_ref[...].reshape(-1, out_ref.shape[0])
    out_ref[...] = dot(mixed, w_ref[...], TN).astype(jnp.bfloat16)


VMEM = pl.BlockSpec(memory_space=pltpu.VMEM)
SMEM = pl.BlockSpec(memory_space=pltpu.SMEM)
HBM = pl.BlockSpec(memory_space=pltpu.HBM)


def call(body, operands, outs, specs=None, scratch=()):
    return pl.pallas_call(
        body,
        in_specs=specs or [VMEM] * len(operands),
        out_specs=[VMEM] * len(outs),
        out_shape=[jax.ShapeDtypeStruct(s, d) for s, d in outs],
        scratch_shapes=list(scratch),
        compiler_params=pltpu.CompilerParams(vmem_limit_bytes=20 * 2**20),
    )(*operands)


def in_hbm(value):
    return pltpu.with_memory_space_constraint(value, pltpu.HBM)


def from_behind(value, by):
    devices = lax.axis_size("sp")
    return lax.ppermute(value, "sp", [(i, i + by) for i in range(devices - by)])


def layer(tokens, norm_gain, w_query, w_key, w_value, w_out):
    rows, width = tokens.shape
    bf16, f32 = jnp.bfloat16, jnp.float32
    sp = lax.axis_index("sp").reshape(1)
    slot = lax.axis_index("tp").reshape(1)
    kv0, s1, s2, s3, normed = call(
        project_kernel,
        (in_hbm(tokens), in_hbm(norm_gain.reshape(1, -1)), in_hbm(w_key), in_hbm(w_value)),
        [
            ((rows, PAIR), bf16),
            ((STEPS + 2 * rows, PAIR), bf16),
            ((STEPS + rows, PAIR), bf16),
            ((rows, PAIR), bf16),
            ((rows, width), bf16),
        ],
        specs=[HBM] * 4,
        scratch=[
            pltpu.VMEM((rows, width), bf16),
            pltpu.VMEM((1, width), f32),
            pltpu.VMEM((GROUPS * PAIR, width), bf16),
            pltpu.SemaphoreType.DMA((rows // CHUNK + 2 * GROUPS + 1,)),
        ],
    )
    r1 = from_behind(s1, 1)
    r2 = from_behind(s2, 2)
    r3 = from_behind(s3, 3)
    (q,) = call(query_kernel, (normed, w_query), [((rows, GROUPS * HEAD_DIM), bf16)])
    (s4,) = call(relay_kernel, (s3, r1, r2), [((STEPS + 2 * rows, PAIR), bf16)])
    r4 = from_behind(s4, 4)
    o, l, e, top, total = call(
        early_kernel,
        (sp, slot, q, kv0, s1, s3, r1, r2, r3),
        [((rows, HEAD_DIM), f32), ((rows, 1), f32), ((rows, rows), f32), ((rows, 1), f32), ((rows, 1), f32)],
        specs=[SMEM] * 2 + [VMEM] * 7,
    )
    devices = lax.axis_size("tp")
    mix, lw = call(
        late_kernel,
        (sp, slot, q, s3, r1, r2, r3, r4, o, l, e, top, total),
        [((devices, HEAD_DIM, rows), bf16), ((rows, 1), f32)],
        specs=[SMEM] * 2 + [VMEM] * 11,
    )
    everyone = lax.all_to_all(mix, "tp", 0, 0, tiled=True)
    (log_weight,) = call(log_weight_kernel, (lw,), [((1, rows), f32)])
    (projected,) = call(output_kernel, (everyone, w_out), [((rows, w_out.shape[1]), bf16)])
    return projected, log_weight


def solution(mesh):
    in_specs = (P("sp", None), P(), P(None, "tp", None), P(None, "tp", None), P(None, "tp", None), P(None, "tp"))
    out_specs = (P("sp", "tp"), P("tp", "sp"))
    return jax.shard_map(layer, mesh=mesh, in_specs=in_specs, out_specs=out_specs, check_vma=False)
```

```python
import jax
import jax.numpy as jnp
from jax import lax
from jax.experimental import pallas as pl
from jax.experimental.pallas import tpu as pltpu
from jax.sharding import PartitionSpec as P


HEAD_DIM = 64
SLOTS = 8
STEPS = 128
GROUPS = 3
WIDE_DILATION = 16
NEG_BIG = -1e30

CLASSES = 4
PAIR = 2 * HEAD_DIM
CHUNK = 128
HALO = STEPS // WIDE_DILATION
NT = (((1,), (1,)), ((), ()))
NN = (((1,), (0,)), ((), ()))
TN = (((0,), (0,)), ((), ()))


def dot(a, b, dims):
    return lax.dot_general(a, b, dims, preferred_element_type=jnp.float32)


def line(length, dim):
    return lax.broadcasted_iota(jnp.int32, (length, 1) if dim == 0 else (1, length), dim)


def split(n, size):
    q = jnp.zeros_like(n)
    for k in range(1, 32):
        q = q + (n >= k * size).astype(jnp.int32)
    return q, n - q * size


def run_of_class(per_class, dim):
    return split(line(per_class, dim), per_class // CLASSES)


def run_of_halo(rows_per_residue, dim):
    j, i = split(line(STEPS // CLASSES, dim), HALO)
    return j, i + rows_per_residue - HALO


def positions(rows, dim):
    j, i = run_of_class(rows // CLASSES, dim)
    return jnp.concatenate([16 * i + 4 * j + c for c in range(CLASSES)], axis=dim)


def to_class_order(rows):
    return positions(rows, 0) == line(rows, 1)


def halo_rows(rows):
    per_residue = rows // WIDE_DILATION
    return [r * per_residue + per_residue - HALO for r in range(WIDE_DILATION)]


def queries(normed, wq_ref):
    wq = wq_ref[...].reshape(GROUPS * HEAD_DIM, -1)
    q = (dot(normed, wq, NT).astype(jnp.bfloat16) * jnp.bfloat16(0.125)).astype(jnp.bfloat16)
    return dot(to_class_order(normed.shape[0]).astype(jnp.bfloat16), q, NN).astype(jnp.bfloat16)


def project_kernel(
    slot_ref, tokens_hbm, gain_hbm, wk_hbm, wv_hbm, wq_hbm, kv0_ref, s1_ref, s2_ref, s3_ref, normed_ref, q_ref, x_ref, gain_ref, w_ref,
    wq_ref, sem,
):
    rows = x_ref.shape[0]
    chunks = rows // CHUNK
    gain_load = pltpu.make_async_copy(gain_hbm, gain_ref, sem.at[chunks + 2 * GROUPS])
    gain_load.start()
    loads = [
        pltpu.make_async_copy(tokens_hbm.at[pl.ds(n * CHUNK, CHUNK)], x_ref.at[pl.ds(n * CHUNK, CHUNK)], sem.at[n])
        for n in range(chunks)
    ]
    for g in range(GROUPS):
        at = chunks + 2 * g
        loads.append(pltpu.make_async_copy(wk_hbm.at[g], w_ref.at[pl.ds(g * PAIR, HEAD_DIM)], sem.at[at]))
        loads.append(
            pltpu.make_async_copy(wv_hbm.at[g], w_ref.at[pl.ds(g * PAIR + HEAD_DIM, HEAD_DIM)], sem.at[at + 1])
        )
    for load in loads:
        load.start()
    wq_load = pltpu.make_async_copy(wq_hbm, wq_ref, sem.at[chunks + 2 * GROUPS + 1])
    wq_load.start()
    pick = to_class_order(rows).astype(jnp.bfloat16)
    gain_load.wait()
    gain = gain_ref[...]
    for n in range(chunks):
        loads[n].wait()
        run = pl.ds(n * CHUNK, CHUNK)
        x = x_ref[run, :].astype(jnp.float32)
        mean = jnp.mean(x * x, axis=-1, keepdims=True)
        normed_ref[run, :] = (x * lax.rsqrt(mean + 1e-6) * gain).astype(jnp.bfloat16)
    for load in loads[chunks:]:
        load.wait()
    kv = dot(normed_ref[...], w_ref[...], NT).astype(jnp.bfloat16)
    kv = dot(pick, kv, NN).astype(jnp.bfloat16)
    kv0_ref[...] = kv[:, 0:PAIR]
    s1_ref[STEPS : STEPS + rows, :] = kv[:, PAIR : 2 * PAIR]
    s1_ref[STEPS + rows : STEPS + 2 * rows, :] = kv[:, 2 * PAIR : 3 * PAIR]
    s2_ref[STEPS : STEPS + rows, :] = kv[:, 2 * PAIR : 3 * PAIR]
    s3_ref[...] = kv[:, 2 * PAIR : 3 * PAIR]
    for r, lo in enumerate(halo_rows(rows)):
        s1_ref[r * HALO : (r + 1) * HALO, :] = kv[lo : lo + HALO, 0:PAIR]
        s2_ref[r * HALO : (r + 1) * HALO, :] = kv[lo : lo + HALO, PAIR : 2 * PAIR]
    wq_load.wait()

    @pl.when(slot_ref[0] % 2 == 1)
    def _():
        q_ref[...] = queries(normed_ref[...], wq_ref)


def query_kernel(slot_ref, normed_ref, wq_ref, done_ref, q_ref):
    @pl.when(slot_ref[0] % 2 == 1)
    def _():
        q_ref[...] = done_ref[...]

    @pl.when(slot_ref[0] % 2 == 0)
    def _():
        q_ref[...] = queries(normed_ref[...], wq_ref)


def relay_kernel(s3_ref, r1_ref, r2_ref, s4_ref):
    rows = s3_ref.shape[0]
    s4_ref[0:rows, :] = s3_ref[...]
    s4_ref[rows : 2 * rows, :] = r1_ref[STEPS + rows : STEPS + 2 * rows, :]
    for r, lo in enumerate(halo_rows(rows)):
        at = 2 * rows + r * HALO
        s4_ref[at : at + HALO, :] = r2_ref[STEPS + lo : STEPS + lo + HALO, :]


def slope_of(group, slot):
    n = jnp.full((1, 1), group * SLOTS + 1, jnp.int32) + slot
    return jnp.exp2(-8.0 * n.astype(jnp.float32) / (GROUPS * SLOTS))


def bias_of(distance, valid, slope):
    ok = valid & (distance >= 0) & (distance <= STEPS)
    return jnp.where(ok, -slope * distance.astype(jnp.float32), NEG_BIG)


def softmax_pieces(scores):
    top = jnp.max(scores, axis=-1, keepdims=True)
    e = jnp.exp(scores - top)
    total = jnp.sum(e, axis=-1, keepdims=True)
    return (e * (1.0 / total)).astype(jnp.bfloat16), top + jnp.log(total)


def wide_bias(rows, blocks, sp, slope, halo_block=None):
    per_class, per_residue = rows // CLASSES, rows // WIDE_DILATION
    jq, iq = run_of_class(per_class, 0)
    jk, ik = run_of_class(per_class, 1)
    js, at, ok = [], [], []
    for b in blocks:
        js.append(jk)
        at.append(ik - per_residue * b)
        ok.append(jnp.full_like(jk, b) <= sp)
    if halo_block is not None:
        jh, ih = run_of_halo(per_residue, 1)
        js.append(jh)
        at.append(ih - per_residue * halo_block)
        ok.append(jnp.full_like(jh, halo_block) <= sp)
    js, at = jnp.concatenate(js, axis=1), jnp.concatenate(at, axis=1)
    ok = jnp.concatenate([o.astype(jnp.int32) for o in ok], axis=1) > 0
    return bias_of(iq - at, (jq == js) & ok, slope)


def early_kernel(
    sp_ref, slot_ref, q_ref, kv0_ref, s1_ref, s3_ref, r1_ref, r2_ref, r3_ref, o_ref, l_ref, e_ref, top_ref, sum_ref
):
    rows = kv0_ref.shape[0]
    sp, slot = sp_ref[0], slot_ref[0]
    per_class, per_residue = rows // CLASSES, rows // WIDE_DILATION
    runs = [pl.ds(c * per_class, per_class) for c in range(CLASSES)]
    jh, ih = run_of_halo(per_residue, 1)
    tail = jnp.concatenate([16 * ih + 4 * jh + c - rows for c in range(CLASSES)], axis=1)
    tk = jnp.concatenate([positions(rows, 1), tail], axis=1)
    bias = bias_of(positions(rows, 0) - tk, (tk >= 0) | (sp >= 1), slope_of(0, slot))
    keys = jnp.concatenate([kv0_ref[...], r1_ref[0:STEPS, :]], axis=0)
    p, l0 = softmax_pieces(dot(q_ref[:, 0:HEAD_DIM], keys[:, 0:HEAD_DIM], NT) + bias)
    o0 = dot(p, keys[:, HEAD_DIM:PAIR], NN)
    jq, iq = run_of_class(per_class, 0)
    jk, ik = run_of_class(per_class, 1)
    own = 4 * ik + jk
    tk = jnp.concatenate([own, own - per_class, 4 * ih + jh - 2 * per_class], axis=1)
    block = jnp.concatenate([jnp.zeros_like(own), jnp.full_like(own, 1), jnp.full_like(jh, 2)], axis=1)
    bias = bias_of(4 * iq + jq - tk, block <= sp, slope_of(1, slot))
    halo = STEPS // CLASSES
    keys = [
        jnp.concatenate(
            [
                s1_ref[pl.ds(STEPS + c * per_class, per_class), :],
                r1_ref[pl.ds(STEPS + c * per_class, per_class), :],
                r2_ref[pl.ds(c * halo, halo), :],
            ],
            axis=0,
        )
        for c in range(CLASSES)
    ]
    scores = [dot(q_ref[runs[c], HEAD_DIM : 2 * HEAD_DIM], keys[c][:, 0:HEAD_DIM], NT) + bias for c in range(CLASSES)]
    p, l1 = softmax_pieces(jnp.concatenate(scores, axis=0))
    o1 = [
        dot(p[c * per_class : (c + 1) * per_class], keys[c][:, HEAD_DIM:PAIR], NN) for c in range(CLASSES)
    ]
    top = jnp.maximum(l0, l1)
    w0, w1 = jnp.exp(l0 - top), jnp.exp(l1 - top)
    both = w0 + w1
    l_ref[...] = top + jnp.log(both)
    both = 1.0 / both
    o_ref[...] = (w0 * both) * o0 + (w1 * both) * jnp.concatenate(o1, axis=0)
    bias = wide_bias(rows, (0, 1, 2, 3), sp, slope_of(2, slot))
    scores = []
    for c in range(CLASSES):
        lo = c * per_class
        keys = jnp.concatenate(
            [
                s3_ref[runs[c], 0:HEAD_DIM],
                r1_ref[pl.ds(STEPS + rows + lo, per_class), 0:HEAD_DIM],
                r2_ref[pl.ds(STEPS + lo, per_class), 0:HEAD_DIM],
                r3_ref[runs[c], 0:HEAD_DIM],
            ],
            axis=0,
        )
        scores.append(dot(q_ref[runs[c], 2 * HEAD_DIM : 3 * HEAD_DIM], keys, NT) + bias)
    scores = jnp.concatenate(scores, axis=0)
    top = jnp.max(scores, axis=-1, keepdims=True)
    e = jnp.exp(scores - top)
    e_ref[...] = e
    top_ref[...] = top
    sum_ref[...] = jnp.sum(e, axis=-1, keepdims=True)


def late_kernel(
    sp_ref, slot_ref, q_ref, s3_ref, r1_ref, r2_ref, r3_ref, r4_ref, o_ref, l_ref, e_ref, top_ref, sum_ref, mix_ref, lw_ref
):
    rows = s3_ref.shape[0]
    sp, slot = sp_ref[0], slot_ref[0]
    per_class = rows // CLASSES
    halo = STEPS // CLASSES
    runs = [pl.ds(c * per_class, per_class) for c in range(CLASSES)]
    bias = wide_bias(rows, (4, 5), sp, slope_of(2, slot), halo_block=6)
    keys = [
        jnp.concatenate(
            [r4_ref[runs[c], :], r4_ref[pl.ds(rows + c * per_class, per_class), :], r4_ref[pl.ds(2 * rows + c * halo, halo), :]],
            axis=0,
        )
        for c in range(CLASSES)
    ]
    scores = jnp.concatenate(
        [dot(q_ref[runs[c], 2 * HEAD_DIM : 3 * HEAD_DIM], keys[c][:, 0:HEAD_DIM], NT) + bias for c in range(CLASSES)], axis=0
    )
    top0 = top_ref[...]
    top = jnp.maximum(top0, jnp.max(scores, axis=-1, keepdims=True))
    e = jnp.exp(scores - top)
    shrink = jnp.exp(top0 - top)
    total = sum_ref[...] * shrink + jnp.sum(e, axis=-1, keepdims=True)
    scale = 1.0 / total
    l2 = top + jnp.log(total)
    p = (e * scale).astype(jnp.bfloat16)
    p_early = (e_ref[...] * (shrink * scale)).astype(jnp.bfloat16)
    out = []
    for c in range(CLASSES):
        lo = c * per_class
        early = jnp.concatenate(
            [
                s3_ref[runs[c], HEAD_DIM:PAIR],
                r1_ref[pl.ds(STEPS + rows + lo, per_class), HEAD_DIM:PAIR],
                r2_ref[pl.ds(STEPS + lo, per_class), HEAD_DIM:PAIR],
                r3_ref[runs[c], HEAD_DIM:PAIR],
            ],
            axis=0,
        )
        out.append(
            dot(p_early[lo : lo + per_class], early, NN) + dot(p[lo : lo + per_class], keys[c][:, HEAD_DIM:PAIR], NN)
        )
    l01 = l_ref[...]
    top = jnp.maximum(l01, l2)
    w01, w2 = jnp.exp(l01 - top), jnp.exp(l2 - top)
    both = w01 + w2
    lw_ref[...] = top + jnp.log(both)
    both = 1.0 / both
    mixed = ((w01 * both) * o_ref[...] + (w2 * both) * jnp.concatenate(out, axis=0)).astype(jnp.bfloat16)
    mix = dot(mixed, to_class_order(rows).astype(jnp.bfloat16), TN).astype(jnp.bfloat16)
    for n in range(mix_ref.shape[0]):
        mix_ref[n] = mix


def output_kernel(mix_ref, w_ref, lw_ref, out_ref, log_weight_ref):
    rows = out_ref.shape[0]
    log_weight_ref[...] = jnp.sum(jnp.where(to_class_order(rows), lw_ref[...], 0.0), axis=0, keepdims=True)
    out_ref[...] = dot(mix_ref[...].reshape(-1, rows), w_ref[...], TN).astype(jnp.bfloat16)


VMEM = pl.BlockSpec(memory_space=pltpu.VMEM)
SMEM = pl.BlockSpec(memory_space=pltpu.SMEM)
HBM = pl.BlockSpec(memory_space=pltpu.HBM)


def call(body, operands, outs, specs=None, scratch=()):
    return pl.pallas_call(
        body,
        in_specs=specs or [VMEM] * len(operands),
        out_specs=[VMEM] * len(outs),
        out_shape=[jax.ShapeDtypeStruct(s, d) for s, d in outs],
        scratch_shapes=list(scratch),
        compiler_params=pltpu.CompilerParams(vmem_limit_bytes=20 * 2**20),
    )(*operands)


def in_hbm(value):
    return pltpu.with_memory_space_constraint(value, pltpu.HBM)


def from_behind(value, by):
    devices = lax.axis_size("sp")
    return lax.ppermute(value, "sp", [(i, i + by) for i in range(devices - by)])


def layer(tokens, norm_gain, w_query, w_key, w_value, w_out):
    rows, width = tokens.shape
    bf16, f32 = jnp.bfloat16, jnp.float32
    sp = lax.axis_index("sp").reshape(1)
    slot = lax.axis_index("tp").reshape(1)
    kv0, s1, s2, s3, normed, q = call(
        project_kernel,
        (slot, in_hbm(tokens), in_hbm(norm_gain.reshape(1, -1)), in_hbm(w_key), in_hbm(w_value), in_hbm(w_query)),
        [
            ((rows, PAIR), bf16),
            ((STEPS + 2 * rows, PAIR), bf16),
            ((STEPS + rows, PAIR), bf16),
            ((rows, PAIR), bf16),
            ((rows, width), bf16),
            ((rows, GROUPS * HEAD_DIM), bf16),
        ],
        specs=[SMEM] + [HBM] * 5,
        scratch=[
            pltpu.VMEM((rows, width), bf16),
            pltpu.VMEM((1, width), f32),
            pltpu.VMEM((GROUPS * PAIR, width), bf16),
            pltpu.VMEM(w_query.shape, bf16),
            pltpu.SemaphoreType.DMA((rows // CHUNK + 2 * GROUPS + 2,)),
        ],
    )
    r1 = from_behind(s1, 1)
    r2 = from_behind(s2, 2)
    r3 = from_behind(s3, 3)
    (q,) = call(
        query_kernel, (slot, normed, w_query, q), [((rows, GROUPS * HEAD_DIM), bf16)], specs=[SMEM] + [VMEM] * 3
    )
    (s4,) = call(relay_kernel, (s3, r1, r2), [((STEPS + 2 * rows, PAIR), bf16)])
    r4 = from_behind(s4, 4)
    o, l, e, top, total = call(
        early_kernel,
        (sp, slot, q, kv0, s1, s3, r1, r2, r3),
        [((rows, HEAD_DIM), f32), ((rows, 1), f32), ((rows, rows), f32), ((rows, 1), f32), ((rows, 1), f32)],
        specs=[SMEM] * 2 + [VMEM] * 7,
    )
    devices = lax.axis_size("tp")
    mix, lw = call(
        late_kernel,
        (sp, slot, q, s3, r1, r2, r3, r4, o, l, e, top, total),
        [((devices, HEAD_DIM, rows), bf16), ((rows, 1), f32)],
        specs=[SMEM] * 2 + [VMEM] * 11,
    )
    everyone = lax.all_to_all(mix, "tp", 0, 0, tiled=True)
    projected, log_weight = call(
        output_kernel, (everyone, w_out, lw), [((rows, w_out.shape[1]), bf16), ((1, rows), f32)]
    )
    return projected, log_weight


def solution(mesh):
    in_specs = (P("sp", None), P(), P(None, "tp", None), P(None, "tp", None), P(None, "tp", None), P(None, "tp"))
    out_specs = (P("sp", "tp"), P("tp", "sp"))
    return jax.shard_map(layer, mesh=mesh, in_specs=in_specs, out_specs=out_specs, check_vma=False)
```

```python
import jax
import jax.numpy as jnp
from jax import lax
from jax.experimental import pallas as pl
from jax.experimental.pallas import tpu as pltpu
from jax.sharding import PartitionSpec as P


HEAD_DIM = 64
SLOTS = 8
STEPS = 128
GROUPS = 3
WIDE_DILATION = 16
NEG_BIG = -1e30

CLASSES = 4
PAIR = 2 * HEAD_DIM
CHUNK = 128
HALO = STEPS // WIDE_DILATION
NT = (((1,), (1,)), ((), ()))
NN = (((1,), (0,)), ((), ()))
TN = (((0,), (0,)), ((), ()))


def dot(a, b, dims):
    return lax.dot_general(a, b, dims, preferred_element_type=jnp.float32)


def line(length, dim):
    return lax.broadcasted_iota(jnp.int32, (length, 1) if dim == 0 else (1, length), dim)


def split(n, size):
    q = jnp.zeros_like(n)
    for k in range(1, 32):
        q = q + (n >= k * size).astype(jnp.int32)
    return q, n - q * size


def run_of_class(per_class, dim):
    return split(line(per_class, dim), per_class // CLASSES)


def run_of_halo(rows_per_residue, dim):
    j, i = split(line(STEPS // CLASSES, dim), HALO)
    return j, i + rows_per_residue - HALO


def positions(rows, dim):
    j, i = run_of_class(rows // CLASSES, dim)
    return jnp.concatenate([16 * i + 4 * j + c for c in range(CLASSES)], axis=dim)


def to_class_order(rows):
    return positions(rows, 0) == line(rows, 1)


def halo_rows(rows):
    per_residue = rows // WIDE_DILATION
    return [r * per_residue + per_residue - HALO for r in range(WIDE_DILATION)]


def project_kernel(
    tokens_hbm, gain_hbm, wk_hbm, wv_hbm, kv0_ref, s1_ref, s2_ref, s3_ref, normed_ref, x_ref, gain_ref, w_ref, sem
):
    rows = x_ref.shape[0]
    chunks = rows // CHUNK
    gain_load = pltpu.make_async_copy(gain_hbm, gain_ref, sem.at[chunks + 2 * GROUPS])
    gain_load.start()
    loads = [
        pltpu.make_async_copy(tokens_hbm.at[pl.ds(n * CHUNK, CHUNK)], x_ref.at[pl.ds(n * CHUNK, CHUNK)], sem.at[n])
        for n in range(chunks)
    ]
    for g in range(GROUPS):
        at = chunks + 2 * g
        loads.append(pltpu.make_async_copy(wk_hbm.at[g], w_ref.at[pl.ds(g * PAIR, HEAD_DIM)], sem.at[at]))
        loads.append(
            pltpu.make_async_copy(wv_hbm.at[g], w_ref.at[pl.ds(g * PAIR + HEAD_DIM, HEAD_DIM)], sem.at[at + 1])
        )
    for load in loads:
        load.start()
    pick = to_class_order(rows).astype(jnp.bfloat16)
    gain_load.wait()
    gain = gain_ref[...]
    for n in range(chunks):
        loads[n].wait()
        run = pl.ds(n * CHUNK, CHUNK)
        x = x_ref[run, :].astype(jnp.float32)
        mean = jnp.mean(x * x, axis=-1, keepdims=True)
        normed_ref[run, :] = (x * lax.rsqrt(mean + 1e-6) * gain).astype(jnp.bfloat16)
    for load in loads[chunks:]:
        load.wait()
    kv = dot(normed_ref[...], w_ref[...], NT).astype(jnp.bfloat16)
    kv = dot(pick, kv, NN).astype(jnp.bfloat16)
    kv0_ref[...] = kv[:, 0:PAIR]
    s1_ref[STEPS : STEPS + rows, :] = kv[:, PAIR : 2 * PAIR]
    s1_ref[STEPS + rows : STEPS + 2 * rows, :] = kv[:, 2 * PAIR : 3 * PAIR]
    s2_ref[STEPS : STEPS + rows, :] = kv[:, 2 * PAIR : 3 * PAIR]
    s3_ref[...] = kv[:, 2 * PAIR : 3 * PAIR]
    for r, lo in enumerate(halo_rows(rows)):
        s1_ref[r * HALO : (r + 1) * HALO, :] = kv[lo : lo + HALO, 0:PAIR]
        s2_ref[r * HALO : (r + 1) * HALO, :] = kv[lo : lo + HALO, PAIR : 2 * PAIR]


def query_kernel(normed_ref, wq_ref, q_ref):
    rows = normed_ref.shape[0]
    wq = wq_ref[...].reshape(GROUPS * HEAD_DIM, -1)
    q = (dot(normed_ref[...], wq, NT).astype(jnp.bfloat16) * jnp.bfloat16(0.125)).astype(jnp.bfloat16)
    q_ref[...] = dot(to_class_order(rows).astype(jnp.bfloat16), q, NN).astype(jnp.bfloat16)


def relay_kernel(s3_ref, r1_ref, r2_ref, s4_ref):
    rows = s3_ref.shape[0]
    s4_ref[0:rows, :] = s3_ref[...]
    s4_ref[rows : 2 * rows, :] = r1_ref[STEPS + rows : STEPS + 2 * rows, :]
    for r, lo in enumerate(halo_rows(rows)):
        at = 2 * rows + r * HALO
        s4_ref[at : at + HALO, :] = r2_ref[STEPS + lo : STEPS + lo + HALO, :]


def slope_of(group, slot):
    n = jnp.full((1, 1), group * SLOTS + 1, jnp.int32) + slot
    return jnp.exp2(-8.0 * n.astype(jnp.float32) / (GROUPS * SLOTS))


def bias_of(distance, valid, slope):
    ok = valid & (distance >= 0) & (distance <= STEPS)
    return jnp.where(ok, -slope * distance.astype(jnp.float32), NEG_BIG)


def softmax_pieces(scores):
    top = jnp.max(scores, axis=-1, keepdims=True)
    e = jnp.exp(scores - top)
    total = jnp.sum(e, axis=-1, keepdims=True)
    return (e * (1.0 / total)).astype(jnp.bfloat16), top + jnp.log(total)


def wide_bias(rows, blocks, sp, slope, halo_block=None):
    per_class, per_residue = rows // CLASSES, rows // WIDE_DILATION
    jq, iq = run_of_class(per_class, 0)
    jk, ik = run_of_class(per_class, 1)
    js, at, ok = [], [], []
    for b in blocks:
        js.append(jk)
        at.append(ik - per_residue * b)
        ok.append(jnp.full_like(jk, b) <= sp)
    if halo_block is not None:
        jh, ih = run_of_halo(per_residue, 1)
        js.append(jh)
        at.append(ih - per_residue * halo_block)
        ok.append(jnp.full_like(jh, halo_block) <= sp)
    js, at = jnp.concatenate(js, axis=1), jnp.concatenate(at, axis=1)
    ok = jnp.concatenate([o.astype(jnp.int32) for o in ok], axis=1) > 0
    return bias_of(iq - at, (jq == js) & ok, slope)


def early_kernel(
    sp_ref, slot_ref, q_ref, kv0_ref, s1_ref, s3_ref, r1_ref, r2_ref, r3_ref, o_ref, l_ref, e_ref, top_ref, sum_ref
):
    rows = kv0_ref.shape[0]
    sp, slot = sp_ref[0], slot_ref[0]
    per_class, per_residue = rows // CLASSES, rows // WIDE_DILATION
    runs = [pl.ds(c * per_class, per_class) for c in range(CLASSES)]
    jh, ih = run_of_halo(per_residue, 1)
    tail = jnp.concatenate([16 * ih + 4 * jh + c - rows for c in range(CLASSES)], axis=1)
    tk = jnp.concatenate([positions(rows, 1), tail], axis=1)
    bias = bias_of(positions(rows, 0) - tk, (tk >= 0) | (sp >= 1), slope_of(0, slot))
    keys = jnp.concatenate([kv0_ref[...], r1_ref[0:STEPS, :]], axis=0)
    p, l0 = softmax_pieces(dot(q_ref[:, 0:HEAD_DIM], keys[:, 0:HEAD_DIM], NT) + bias)
    o0 = dot(p, keys[:, HEAD_DIM:PAIR], NN)
    jq, iq = run_of_class(per_class, 0)
    jk, ik = run_of_class(per_class, 1)
    own = 4 * ik + jk
    tk = jnp.concatenate([own, own - per_class, 4 * ih + jh - 2 * per_class], axis=1)
    block = jnp.concatenate([jnp.zeros_like(own), jnp.full_like(own, 1), jnp.full_like(jh, 2)], axis=1)
    bias = bias_of(4 * iq + jq - tk, block <= sp, slope_of(1, slot))
    halo = STEPS // CLASSES
    keys = [
        jnp.concatenate(
            [
                s1_ref[pl.ds(STEPS + c * per_class, per_class), :],
                r1_ref[pl.ds(STEPS + c * per_class, per_class), :],
                r2_ref[pl.ds(c * halo, halo), :],
            ],
            axis=0,
        )
        for c in range(CLASSES)
    ]
    scores = [dot(q_ref[runs[c], HEAD_DIM : 2 * HEAD_DIM], keys[c][:, 0:HEAD_DIM], NT) + bias for c in range(CLASSES)]
    p, l1 = softmax_pieces(jnp.concatenate(scores, axis=0))
    o1 = [
        dot(p[c * per_class : (c + 1) * per_class], keys[c][:, HEAD_DIM:PAIR], NN) for c in range(CLASSES)
    ]
    top = jnp.maximum(l0, l1)
    w0, w1 = jnp.exp(l0 - top), jnp.exp(l1 - top)
    both = w0 + w1
    l_ref[...] = top + jnp.log(both)
    both = 1.0 / both
    o_ref[...] = (w0 * both) * o0 + (w1 * both) * jnp.concatenate(o1, axis=0)
    bias = wide_bias(rows, (0, 1, 2, 3), sp, slope_of(2, slot))
    scores = []
    for c in range(CLASSES):
        lo = c * per_class
        keys = jnp.concatenate(
            [
                s3_ref[runs[c], 0:HEAD_DIM],
                r1_ref[pl.ds(STEPS + rows + lo, per_class), 0:HEAD_DIM],
                r2_ref[pl.ds(STEPS + lo, per_class), 0:HEAD_DIM],
                r3_ref[runs[c], 0:HEAD_DIM],
            ],
            axis=0,
        )
        scores.append(dot(q_ref[runs[c], 2 * HEAD_DIM : 3 * HEAD_DIM], keys, NT) + bias)
    scores = jnp.concatenate(scores, axis=0)
    top = jnp.max(scores, axis=-1, keepdims=True)
    e = jnp.exp(scores - top)
    e_ref[...] = e
    top_ref[...] = top
    sum_ref[...] = jnp.sum(e, axis=-1, keepdims=True)


def late_kernel(
    sp_ref, slot_ref, q_ref, s3_ref, r1_ref, r2_ref, r3_ref, r4_ref, o_ref, l_ref, e_ref, top_ref, sum_ref, mix_ref, lw_ref
):
    rows = s3_ref.shape[0]
    sp, slot = sp_ref[0], slot_ref[0]
    per_class = rows // CLASSES
    halo = STEPS // CLASSES
    runs = [pl.ds(c * per_class, per_class) for c in range(CLASSES)]
    bias = wide_bias(rows, (4, 5), sp, slope_of(2, slot), halo_block=6)
    keys = [
        jnp.concatenate(
            [r4_ref[runs[c], :], r4_ref[pl.ds(rows + c * per_class, per_class), :], r4_ref[pl.ds(2 * rows + c * halo, halo), :]],
            axis=0,
        )
        for c in range(CLASSES)
    ]
    scores = jnp.concatenate(
        [dot(q_ref[runs[c], 2 * HEAD_DIM : 3 * HEAD_DIM], keys[c][:, 0:HEAD_DIM], NT) + bias for c in range(CLASSES)], axis=0
    )
    top0 = top_ref[...]
    top = jnp.maximum(top0, jnp.max(scores, axis=-1, keepdims=True))
    e = jnp.exp(scores - top)
    shrink = jnp.exp(top0 - top)
    total = sum_ref[...] * shrink + jnp.sum(e, axis=-1, keepdims=True)
    scale = 1.0 / total
    l2 = top + jnp.log(total)
    p = (e * scale).astype(jnp.bfloat16)
    p_early = (e_ref[...] * (shrink * scale)).astype(jnp.bfloat16)
    out = []
    for c in range(CLASSES):
        lo = c * per_class
        early = jnp.concatenate(
            [
                s3_ref[runs[c], HEAD_DIM:PAIR],
                r1_ref[pl.ds(STEPS + rows + lo, per_class), HEAD_DIM:PAIR],
                r2_ref[pl.ds(STEPS + lo, per_class), HEAD_DIM:PAIR],
                r3_ref[runs[c], HEAD_DIM:PAIR],
            ],
            axis=0,
        )
        out.append(
            dot(p_early[lo : lo + per_class], early, NN) + dot(p[lo : lo + per_class], keys[c][:, HEAD_DIM:PAIR], NN)
        )
    l01 = l_ref[...]
    top = jnp.maximum(l01, l2)
    w01, w2 = jnp.exp(l01 - top), jnp.exp(l2 - top)
    both = w01 + w2
    lw_ref[...] = top + jnp.log(both)
    both = 1.0 / both
    mixed = ((w01 * both) * o_ref[...] + (w2 * both) * jnp.concatenate(out, axis=0)).astype(jnp.bfloat16)
    mix = dot(mixed, to_class_order(rows).astype(jnp.bfloat16), TN).astype(jnp.bfloat16)
    for n in range(mix_ref.shape[0]):
        mix_ref[n] = mix


def output_kernel(mix_ref, w_ref, lw_ref, out_ref, log_weight_ref):
    rows = out_ref.shape[0]
    log_weight_ref[...] = jnp.sum(jnp.where(to_class_order(rows), lw_ref[...], 0.0), axis=0, keepdims=True)
    out_ref[...] = dot(mix_ref[...].reshape(-1, rows), w_ref[...], TN).astype(jnp.bfloat16)


VMEM = pl.BlockSpec(memory_space=pltpu.VMEM)
SMEM = pl.BlockSpec(memory_space=pltpu.SMEM)
HBM = pl.BlockSpec(memory_space=pltpu.HBM)


def call(body, operands, outs, specs=None, scratch=()):
    return pl.pallas_call(
        body,
        in_specs=specs or [VMEM] * len(operands),
        out_specs=[VMEM] * len(outs),
        out_shape=[jax.ShapeDtypeStruct(s, d) for s, d in outs],
        scratch_shapes=list(scratch),
        compiler_params=pltpu.CompilerParams(vmem_limit_bytes=20 * 2**20),
    )(*operands)


def in_hbm(value):
    return pltpu.with_memory_space_constraint(value, pltpu.HBM)


def from_behind(value, by):
    devices = lax.axis_size("sp")
    return lax.ppermute(value, "sp", [(i, i + by) for i in range(devices - by)])


def layer(tokens, norm_gain, w_query, w_key, w_value, w_out):
    rows, width = tokens.shape
    bf16, f32 = jnp.bfloat16, jnp.float32
    sp = lax.axis_index("sp").reshape(1)
    slot = lax.axis_index("tp").reshape(1)
    kv0, s1, s2, s3, normed = call(
        project_kernel,
        (in_hbm(tokens), in_hbm(norm_gain.reshape(1, -1)), in_hbm(w_key), in_hbm(w_value)),
        [
            ((rows, PAIR), bf16),
            ((STEPS + 2 * rows, PAIR), bf16),
            ((STEPS + rows, PAIR), bf16),
            ((rows, PAIR), bf16),
            ((rows, width), bf16),
        ],
        specs=[HBM] * 4,
        scratch=[
            pltpu.VMEM((rows, width), bf16),
            pltpu.VMEM((1, width), f32),
            pltpu.VMEM((GROUPS * PAIR, width), bf16),
            pltpu.SemaphoreType.DMA((rows // CHUNK + 2 * GROUPS + 1,)),
        ],
    )
    r1 = from_behind(s1, 1)
    r2 = from_behind(s2, 2)
    r3 = from_behind(s3, 3)
    (q,) = call(query_kernel, (normed, w_query), [((rows, GROUPS * HEAD_DIM), bf16)])
    (s4,) = call(relay_kernel, (s3, r1, r2), [((STEPS + 2 * rows, PAIR), bf16)])
    r4 = from_behind(s4, 4)
    o, l, e, top, total = call(
        early_kernel,
        (sp, slot, q, kv0, s1, s3, r1, r2, r3),
        [((rows, HEAD_DIM), f32), ((rows, 1), f32), ((rows, rows), f32), ((rows, 1), f32), ((rows, 1), f32)],
        specs=[SMEM] * 2 + [VMEM] * 7,
    )
    devices = lax.axis_size("tp")
    mix, lw = call(
        late_kernel,
        (sp, slot, q, s3, r1, r2, r3, r4, o, l, e, top, total),
        [((devices, HEAD_DIM, rows), bf16), ((rows, 1), f32)],
        specs=[SMEM] * 2 + [VMEM] * 11,
    )
    everyone = lax.all_to_all(mix, "tp", 0, 0, tiled=True)
    projected, log_weight = call(
        output_kernel, (everyone, w_out, lw), [((rows, w_out.shape[1]), bf16), ((1, rows), f32)]
    )
    return projected, log_weight


def solution(mesh):
    in_specs = (P("sp", None), P(), P(None, "tp", None), P(None, "tp", None), P(None, "tp", None), P(None, "tp"))
    out_specs = (P("sp", "tp"), P("tp", "sp"))
    return jax.shard_map(layer, mesh=mesh, in_specs=in_specs, out_specs=out_specs, check_vma=False)
```

```python
import jax
import jax.numpy as jnp
from jax import lax
from jax.experimental import pallas as pl
from jax.experimental.pallas import tpu as pltpu
from jax.sharding import PartitionSpec as P


HEAD_DIM = 64
SLOTS = 8
STEPS = 128
GROUPS = 3
WIDE_DILATION = 16
NEG_BIG = -1e30

CLASSES = 4
PAIR = 2 * HEAD_DIM
CHUNK = 128
HALO = STEPS // WIDE_DILATION
NT = (((1,), (1,)), ((), ()))
NN = (((1,), (0,)), ((), ()))
TN = (((0,), (0,)), ((), ()))


def dot(a, b, dims):
    return lax.dot_general(a, b, dims, preferred_element_type=jnp.float32)


def line(length, dim):
    return lax.broadcasted_iota(jnp.int32, (length, 1) if dim == 0 else (1, length), dim)


def split(n, size):
    q = jnp.zeros_like(n)
    for k in range(1, 32):
        q = q + (n >= k * size).astype(jnp.int32)
    return q, n - q * size


def run_of_class(per_class, dim):
    return split(line(per_class, dim), per_class // CLASSES)


def run_of_halo(rows_per_residue, dim):
    j, i = split(line(STEPS // CLASSES, dim), HALO)
    return j, i + rows_per_residue - HALO


def positions(rows, dim):
    j, i = run_of_class(rows // CLASSES, dim)
    return jnp.concatenate([16 * i + 4 * j + c for c in range(CLASSES)], axis=dim)


def to_class_order(rows):
    return positions(rows, 0) == line(rows, 1)


def halo_rows(rows):
    per_residue = rows // WIDE_DILATION
    return [r * per_residue + per_residue - HALO for r in range(WIDE_DILATION)]


def project_kernel(
    tokens_hbm, gain_hbm, wk_hbm, wv_hbm, kv0_ref, s1_ref, s2_ref, s3_ref, normed_ref, x_ref, gain_ref, w_ref, sem
):
    rows = x_ref.shape[0]
    chunks = rows // CHUNK
    gain_load = pltpu.make_async_copy(gain_hbm, gain_ref, sem.at[chunks + 2 * GROUPS])
    gain_load.start()
    loads = [
        pltpu.make_async_copy(tokens_hbm.at[pl.ds(n * CHUNK, CHUNK)], x_ref.at[pl.ds(n * CHUNK, CHUNK)], sem.at[n])
        for n in range(chunks)
    ]
    for g in range(GROUPS):
        at = chunks + 2 * g
        loads.append(pltpu.make_async_copy(wk_hbm.at[g], w_ref.at[pl.ds(g * PAIR, HEAD_DIM)], sem.at[at]))
        loads.append(
            pltpu.make_async_copy(wv_hbm.at[g], w_ref.at[pl.ds(g * PAIR + HEAD_DIM, HEAD_DIM)], sem.at[at + 1])
        )
    for load in loads:
        load.start()
    pick = to_class_order(rows).astype(jnp.bfloat16)
    gain_load.wait()
    gain = gain_ref[...]
    for n in range(chunks):
        loads[n].wait()
        run = pl.ds(n * CHUNK, CHUNK)
        x = x_ref[run, :].astype(jnp.float32)
        mean = jnp.mean(x * x, axis=-1, keepdims=True)
        normed_ref[run, :] = (x * lax.rsqrt(mean + 1e-6) * gain).astype(jnp.bfloat16)
    for load in loads[chunks:]:
        load.wait()
    kv = dot(normed_ref[...], w_ref[...], NT).astype(jnp.bfloat16)
    kv = dot(pick, kv, NN).astype(jnp.bfloat16)
    kv0_ref[...] = kv[:, 0:PAIR]
    s1_ref[STEPS : STEPS + rows, :] = kv[:, PAIR : 2 * PAIR]
    s1_ref[STEPS + rows : STEPS + 2 * rows, :] = kv[:, 2 * PAIR : 3 * PAIR]
    s2_ref[STEPS : STEPS + rows, :] = kv[:, 2 * PAIR : 3 * PAIR]
    s3_ref[...] = kv[:, 2 * PAIR : 3 * PAIR]
    for r, lo in enumerate(halo_rows(rows)):
        s1_ref[r * HALO : (r + 1) * HALO, :] = kv[lo : lo + HALO, 0:PAIR]
        s2_ref[r * HALO : (r + 1) * HALO, :] = kv[lo : lo + HALO, PAIR : 2 * PAIR]


def query_kernel(normed_ref, wq_ref, q_ref):
    rows = normed_ref.shape[0]
    wq = wq_ref[...].reshape(GROUPS * HEAD_DIM, -1)
    q = (dot(normed_ref[...], wq, NT).astype(jnp.bfloat16) * jnp.bfloat16(0.125)).astype(jnp.bfloat16)
    q_ref[...] = dot(to_class_order(rows).astype(jnp.bfloat16), q, NN).astype(jnp.bfloat16)


def relay_kernel(r1_ref, r2_ref, s4_ref):
    rows = r1_ref.shape[0] // 2 - STEPS // 2
    s4_ref[0:rows, :] = r1_ref[STEPS + rows : STEPS + 2 * rows, :]
    for r, lo in enumerate(halo_rows(rows)):
        at = rows + r * HALO
        s4_ref[at : at + HALO, :] = r2_ref[STEPS + lo : STEPS + lo + HALO, :]


def slope_of(group, slot):
    n = jnp.full((1, 1), group * SLOTS + 1, jnp.int32) + slot
    return jnp.exp2(-8.0 * n.astype(jnp.float32) / (GROUPS * SLOTS))


def bias_of(at_query, at_key, valid, slope, same=None):
    at_key = jnp.where(valid, at_key.astype(jnp.float32), 1e9)
    distance = at_query.astype(jnp.float32) - at_key
    ok = jnp.abs(distance - STEPS / 2) <= STEPS / 2
    return jnp.where(ok if same is None else ok & same, -slope * distance, NEG_BIG)


def softmax_pieces(scores):
    top = jnp.max(scores, axis=-1, keepdims=True)
    e = jnp.exp(scores - top)
    total = jnp.sum(e, axis=-1, keepdims=True)
    return (e * (1.0 / total)).astype(jnp.bfloat16), top + jnp.log(total)


def wide_bias(rows, blocks, sp, slope, halo_block=None):
    per_class, per_residue = rows // CLASSES, rows // WIDE_DILATION
    jq, iq = run_of_class(per_class, 0)
    jk, ik = run_of_class(per_class, 1)
    js, at, ok = [], [], []
    for b in blocks:
        js.append(jk)
        at.append(ik - per_residue * b)
        ok.append(jnp.full_like(jk, b) <= sp)
    if halo_block is not None:
        jh, ih = run_of_halo(per_residue, 1)
        js.append(jh)
        at.append(ih - per_residue * halo_block)
        ok.append(jnp.full_like(jh, halo_block) <= sp)
    js, at = jnp.concatenate(js, axis=1), jnp.concatenate(at, axis=1)
    ok = jnp.concatenate([o.astype(jnp.int32) for o in ok], axis=1) > 0
    return bias_of(iq, at, ok, slope, jq == js)


def early_kernel(
    sp_ref, slot_ref, q_ref, kv0_ref, s1_ref, s3_ref, r1_ref, r2_ref, r3_ref, r4_ref, o_ref, l_ref, e_ref, top_ref,
    sum_ref,
):
    rows = kv0_ref.shape[0]
    sp, slot = sp_ref[0], slot_ref[0]
    per_class, per_residue = rows // CLASSES, rows // WIDE_DILATION
    runs = [pl.ds(c * per_class, per_class) for c in range(CLASSES)]
    jh, ih = run_of_halo(per_residue, 1)
    tail = jnp.concatenate([16 * ih + 4 * jh + c - rows for c in range(CLASSES)], axis=1)
    tk = jnp.concatenate([positions(rows, 1), tail], axis=1)
    bias = bias_of(positions(rows, 0), tk, (tk >= 0) | (sp >= 1), slope_of(0, slot))
    keys = jnp.concatenate([kv0_ref[...], r1_ref[0:STEPS, :]], axis=0)
    p, l0 = softmax_pieces(dot(q_ref[:, 0:HEAD_DIM], keys[:, 0:HEAD_DIM], NT) + bias)
    o0 = dot(p, keys[:, HEAD_DIM:PAIR], NN)
    jq, iq = run_of_class(per_class, 0)
    jk, ik = run_of_class(per_class, 1)
    own = 4 * ik + jk
    tk = jnp.concatenate([own, own - per_class, 4 * ih + jh - 2 * per_class], axis=1)
    block = jnp.concatenate([jnp.zeros_like(own), jnp.full_like(own, 1), jnp.full_like(jh, 2)], axis=1)
    bias = bias_of(4 * iq + jq, tk, block <= sp, slope_of(1, slot))
    halo = STEPS // CLASSES
    keys = [
        jnp.concatenate(
            [
                s1_ref[pl.ds(STEPS + c * per_class, per_class), :],
                r1_ref[pl.ds(STEPS + c * per_class, per_class), :],
                r2_ref[pl.ds(c * halo, halo), :],
            ],
            axis=0,
        )
        for c in range(CLASSES)
    ]
    scores = [dot(q_ref[runs[c], HEAD_DIM : 2 * HEAD_DIM], keys[c][:, 0:HEAD_DIM], NT) + bias for c in range(CLASSES)]
    p, l1 = softmax_pieces(jnp.concatenate(scores, axis=0))
    o1 = [
        dot(p[c * per_class : (c + 1) * per_class], keys[c][:, HEAD_DIM:PAIR], NN) for c in range(CLASSES)
    ]
    top = jnp.maximum(l0, l1)
    w0, w1 = jnp.exp(l0 - top), jnp.exp(l1 - top)
    both = w0 + w1
    l_ref[...] = top + jnp.log(both)
    both = 1.0 / both
    o_ref[...] = (w0 * both) * o0 + (w1 * both) * jnp.concatenate(o1, axis=0)
    bias = wide_bias(rows, (0, 1, 2, 3, 4), sp, slope_of(2, slot))
    scores = []
    for c in range(CLASSES):
        lo = c * per_class
        keys = jnp.concatenate(
            [
                s3_ref[runs[c], 0:HEAD_DIM],
                r1_ref[pl.ds(STEPS + rows + lo, per_class), 0:HEAD_DIM],
                r2_ref[pl.ds(STEPS + lo, per_class), 0:HEAD_DIM],
                r3_ref[runs[c], 0:HEAD_DIM],
                r4_ref[runs[c], 0:HEAD_DIM],
            ],
            axis=0,
        )
        scores.append(dot(q_ref[runs[c], 2 * HEAD_DIM : 3 * HEAD_DIM], keys, NT) + bias)
    scores = jnp.concatenate(scores, axis=0)
    top = jnp.max(scores, axis=-1, keepdims=True)
    e = jnp.exp(scores - top)
    e_ref[...] = e
    top_ref[...] = top
    sum_ref[...] = jnp.sum(e, axis=-1, keepdims=True)


def late_kernel(
    sp_ref, slot_ref, q_ref, s3_ref, r1_ref, r2_ref, r3_ref, r4_ref, far_ref, o_ref, l_ref, e_ref, top_ref, sum_ref,
    mix_ref, lw_ref,
):
    rows = s3_ref.shape[0]
    sp, slot = sp_ref[0], slot_ref[0]
    per_class = rows // CLASSES
    halo = STEPS // CLASSES
    runs = [pl.ds(c * per_class, per_class) for c in range(CLASSES)]
    bias = wide_bias(rows, (5,), sp, slope_of(2, slot), halo_block=6)
    keys = [
        jnp.concatenate(
            [far_ref[runs[c], :], far_ref[pl.ds(rows + c * halo, halo), :]],
            axis=0,
        )
        for c in range(CLASSES)
    ]
    scores = jnp.concatenate(
        [dot(q_ref[runs[c], 2 * HEAD_DIM : 3 * HEAD_DIM], keys[c][:, 0:HEAD_DIM], NT) + bias for c in range(CLASSES)], axis=0
    )
    top0 = top_ref[...]
    top = jnp.maximum(top0, jnp.max(scores, axis=-1, keepdims=True))
    e = jnp.exp(scores - top)
    shrink = jnp.exp(top0 - top)
    total = sum_ref[...] * shrink + jnp.sum(e, axis=-1, keepdims=True)
    scale = 1.0 / total
    l2 = top + jnp.log(total)
    p = (e * scale).astype(jnp.bfloat16)
    p_early = (e_ref[...] * (shrink * scale)).astype(jnp.bfloat16)
    out = []
    for c in range(CLASSES):
        lo = c * per_class
        early = jnp.concatenate(
            [
                s3_ref[runs[c], HEAD_DIM:PAIR],
                r1_ref[pl.ds(STEPS + rows + lo, per_class), HEAD_DIM:PAIR],
                r2_ref[pl.ds(STEPS + lo, per_class), HEAD_DIM:PAIR],
                r3_ref[runs[c], HEAD_DIM:PAIR],
                r4_ref[runs[c], HEAD_DIM:PAIR],
            ],
            axis=0,
        )
        out.append(
            dot(p_early[lo : lo + per_class], early, NN) + dot(p[lo : lo + per_class], keys[c][:, HEAD_DIM:PAIR], NN)
        )
    l01 = l_ref[...]
    top = jnp.maximum(l01, l2)
    w01, w2 = jnp.exp(l01 - top), jnp.exp(l2 - top)
    both = w01 + w2
    lw_ref[...] = top + jnp.log(both)
    both = 1.0 / both
    mixed = ((w01 * both) * o_ref[...] + (w2 * both) * jnp.concatenate(out, axis=0)).astype(jnp.bfloat16)
    pick = to_class_order(rows)
    mix = dot(mixed, pick.astype(jnp.bfloat16), TN).astype(jnp.bfloat16)
    for n in range(mix_ref.shape[0]):
        mix_ref[n] = mix


def output_kernel(mix_ref, w_ref, lw_ref, out_ref, log_weight_ref):
    rows = out_ref.shape[0]
    log_weight_ref[...] = jnp.sum(jnp.where(to_class_order(rows), lw_ref[...], 0.0), axis=0, keepdims=True)
    out_ref[...] = dot(mix_ref[...].reshape(-1, rows), w_ref[...], TN).astype(jnp.bfloat16)


VMEM = pl.BlockSpec(memory_space=pltpu.VMEM)
SMEM = pl.BlockSpec(memory_space=pltpu.SMEM)
HBM = pl.BlockSpec(memory_space=pltpu.HBM)


def call(body, operands, outs, specs=None, scratch=()):
    return pl.pallas_call(
        body,
        in_specs=specs or [VMEM] * len(operands),
        out_specs=[VMEM] * len(outs),
        out_shape=[jax.ShapeDtypeStruct(s, d) for s, d in outs],
        scratch_shapes=list(scratch),
        compiler_params=pltpu.CompilerParams(vmem_limit_bytes=20 * 2**20),
    )(*operands)


def in_hbm(value):
    return pltpu.with_memory_space_constraint(value, pltpu.HBM)


def from_behind(value, by):
    devices = lax.axis_size("sp")
    return lax.ppermute(value, "sp", [(i, i + by) for i in range(devices - by)])


def layer(tokens, norm_gain, w_query, w_key, w_value, w_out):
    rows, width = tokens.shape
    bf16, f32 = jnp.bfloat16, jnp.float32
    sp = lax.axis_index("sp").reshape(1)
    slot = lax.axis_index("tp").reshape(1)
    kv0, s1, s2, s3, normed = call(
        project_kernel,
        (in_hbm(tokens), in_hbm(norm_gain.reshape(1, -1)), in_hbm(w_key), in_hbm(w_value)),
        [
            ((rows, PAIR), bf16),
            ((STEPS + 2 * rows, PAIR), bf16),
            ((STEPS + rows, PAIR), bf16),
            ((rows, PAIR), bf16),
            ((rows, width), bf16),
        ],
        specs=[HBM] * 4,
        scratch=[
            pltpu.VMEM((rows, width), bf16),
            pltpu.VMEM((1, width), f32),
            pltpu.VMEM((GROUPS * PAIR, width), bf16),
            pltpu.SemaphoreType.DMA((rows // CHUNK + 2 * GROUPS + 1,)),
        ],
    )
    r1 = from_behind(s1, 1)
    r2 = from_behind(s2, 2)
    r3 = from_behind(s3, 3)
    r4 = from_behind(s3, 4)
    (q,) = call(query_kernel, (normed, w_query), [((rows, GROUPS * HEAD_DIM), bf16)])
    (s4,) = call(relay_kernel, (r1, r2), [((STEPS + rows, PAIR), bf16)])
    far = from_behind(s4, 4)
    o, l, e, top, total = call(
        early_kernel,
        (sp, slot, q, kv0, s1, s3, r1, r2, r3, r4),
        [((rows, HEAD_DIM), f32), ((rows, 1), f32), ((rows, 5 * rows // CLASSES), f32), ((rows, 1), f32), ((rows, 1), f32)],
        specs=[SMEM] * 2 + [VMEM] * 8,
    )
    devices = lax.axis_size("tp")
    mix, lw = call(
        late_kernel,
        (sp, slot, q, s3, r1, r2, r3, r4, far, o, l, e, top, total),
        [((devices, HEAD_DIM, rows), bf16), ((rows, 1), f32)],
        specs=[SMEM] * 2 + [VMEM] * 12,
    )
    everyone = lax.all_to_all(mix, "tp", 0, 0, tiled=True)
    projected, log_weight = call(
        output_kernel, (everyone, w_out, lw), [((rows, w_out.shape[1]), bf16), ((1, rows), f32)]
    )
    return projected, log_weight


def solution(mesh):
    in_specs = (P("sp", None), P(), P(None, "tp", None), P(None, "tp", None), P(None, "tp", None), P(None, "tp"))
    out_specs = (P("sp", "tp"), P("tp", "sp"))
    return jax.shard_map(layer, mesh=mesh, in_specs=in_specs, out_specs=out_specs, check_vma=False)
```

```python
import jax
import jax.numpy as jnp
from jax import lax
from jax.experimental import pallas as pl
from jax.experimental.pallas import tpu as pltpu
from jax.sharding import PartitionSpec as P


HEAD_DIM = 64
SLOTS = 8
STEPS = 128
GROUPS = 3
WIDE_DILATION = 16
NEG_BIG = -1e30

CLASSES = 4
PAIR = 2 * HEAD_DIM
CHUNK = 128
HALO = STEPS // WIDE_DILATION
NT = (((1,), (1,)), ((), ()))
NN = (((1,), (0,)), ((), ()))
TN = (((0,), (0,)), ((), ()))


def dot(a, b, dims):
    return lax.dot_general(a, b, dims, preferred_element_type=jnp.float32)


def line(length, dim):
    return lax.broadcasted_iota(jnp.int32, (length, 1) if dim == 0 else (1, length), dim)


def split(n, size):
    q = jnp.zeros_like(n)
    for k in range(1, 32):
        q = q + (n >= k * size).astype(jnp.int32)
    return q, n - q * size


def run_of_class(per_class, dim):
    return split(line(per_class, dim), per_class // CLASSES)


def run_of_halo(rows_per_residue, dim):
    j, i = split(line(STEPS // CLASSES, dim), HALO)
    return j, i + rows_per_residue - HALO


def positions(rows, dim):
    j, i = run_of_class(rows // CLASSES, dim)
    return jnp.concatenate([16 * i + 4 * j + c for c in range(CLASSES)], axis=dim)


def to_class_order(rows):
    return positions(rows, 0) == line(rows, 1)


def halo_rows(rows):
    per_residue = rows // WIDE_DILATION
    return [r * per_residue + per_residue - HALO for r in range(WIDE_DILATION)]


def project_kernel(
    tokens_hbm, gain_hbm, wk_hbm, wv_hbm, kv0_ref, s1_ref, s2_ref, s3_ref, normed_ref, x_ref, gain_ref, w_ref, sem
):
    rows = x_ref.shape[0]
    chunks = rows // CHUNK
    gain_load = pltpu.make_async_copy(gain_hbm, gain_ref, sem.at[chunks + 2 * GROUPS])
    gain_load.start()
    loads = [
        pltpu.make_async_copy(tokens_hbm.at[pl.ds(n * CHUNK, CHUNK)], x_ref.at[pl.ds(n * CHUNK, CHUNK)], sem.at[n])
        for n in range(chunks)
    ]
    for g in range(GROUPS):
        at = chunks + 2 * g
        loads.append(pltpu.make_async_copy(wk_hbm.at[g], w_ref.at[pl.ds(g * PAIR, HEAD_DIM)], sem.at[at]))
        loads.append(
            pltpu.make_async_copy(wv_hbm.at[g], w_ref.at[pl.ds(g * PAIR + HEAD_DIM, HEAD_DIM)], sem.at[at + 1])
        )
    for load in loads:
        load.start()
    pick = to_class_order(rows).astype(jnp.bfloat16)
    gain_load.wait()
    gain = gain_ref[...]
    for n in range(chunks):
        loads[n].wait()
        run = pl.ds(n * CHUNK, CHUNK)
        x = x_ref[run, :].astype(jnp.float32)
        mean = jnp.mean(x * x, axis=-1, keepdims=True)
        normed_ref[run, :] = (x * lax.rsqrt(mean + 1e-6) * gain).astype(jnp.bfloat16)
    for load in loads[chunks:]:
        load.wait()
    kv = dot(normed_ref[...], w_ref[...], NT).astype(jnp.bfloat16)
    kv = dot(pick, kv, NN).astype(jnp.bfloat16)
    kv0_ref[...] = kv[:, 0:PAIR]
    s1_ref[STEPS : STEPS + rows, :] = kv[:, PAIR : 2 * PAIR]
    s1_ref[STEPS + rows : STEPS + 2 * rows, :] = kv[:, 2 * PAIR : 3 * PAIR]
    s2_ref[STEPS : STEPS + rows, :] = kv[:, 2 * PAIR : 3 * PAIR]
    s3_ref[...] = kv[:, 2 * PAIR : 3 * PAIR]
    for r, lo in enumerate(halo_rows(rows)):
        s1_ref[r * HALO : (r + 1) * HALO, :] = kv[lo : lo + HALO, 0:PAIR]
        s2_ref[r * HALO : (r + 1) * HALO, :] = kv[lo : lo + HALO, PAIR : 2 * PAIR]


def query_kernel(normed_ref, wq_ref, q_ref):
    rows = normed_ref.shape[0]
    wq = wq_ref[...].reshape(GROUPS * HEAD_DIM, -1)
    q = (dot(normed_ref[...], wq, NT).astype(jnp.bfloat16) * jnp.bfloat16(0.125)).astype(jnp.bfloat16)
    q_ref[...] = dot(to_class_order(rows).astype(jnp.bfloat16), q, NN).astype(jnp.bfloat16)


def relay_kernel(s3_ref, r1_ref, r2_ref, s4_ref):
    rows = s3_ref.shape[0]
    s4_ref[0:rows, :] = s3_ref[...]
    s4_ref[rows : 2 * rows, :] = r1_ref[STEPS + rows : STEPS + 2 * rows, :]
    for r, lo in enumerate(halo_rows(rows)):
        at = 2 * rows + r * HALO
        s4_ref[at : at + HALO, :] = r2_ref[STEPS + lo : STEPS + lo + HALO, :]


def slope_of(group, slot):
    n = jnp.full((1, 1), group * SLOTS + 1, jnp.int32) + slot
    return jnp.exp2(-8.0 * n.astype(jnp.float32) / (GROUPS * SLOTS))


def bias_of(at_query, at_key, valid, slope, same=None):
    at_key = jnp.where(valid, at_key.astype(jnp.float32), 1e9)
    distance = at_query.astype(jnp.float32) - at_key
    ok = jnp.abs(distance - STEPS / 2) <= STEPS / 2
    return jnp.where(ok if same is None else ok & same, -slope * distance, NEG_BIG)


def softmax_pieces(scores):
    top = jnp.max(scores, axis=-1, keepdims=True)
    e = jnp.exp(scores - top)
    total = jnp.sum(e, axis=-1, keepdims=True)
    return (e * (1.0 / total)).astype(jnp.bfloat16), top + jnp.log(total)


def wide_bias(rows, blocks, sp, slope, halo_block=None):
    per_class, per_residue = rows // CLASSES, rows // WIDE_DILATION
    jq, iq = run_of_class(per_class, 0)
    jk, ik = run_of_class(per_class, 1)
    js, at, ok = [], [], []
    for b in blocks:
        js.append(jk)
        at.append(ik - per_residue * b)
        ok.append(jnp.full_like(jk, b) <= sp)
    if halo_block is not None:
        jh, ih = run_of_halo(per_residue, 1)
        js.append(jh)
        at.append(ih - per_residue * halo_block)
        ok.append(jnp.full_like(jh, halo_block) <= sp)
    js, at = jnp.concatenate(js, axis=1), jnp.concatenate(at, axis=1)
    ok = jnp.concatenate([o.astype(jnp.int32) for o in ok], axis=1) > 0
    return bias_of(iq, at, ok, slope, jq == js)


def early_kernel(
    sp_ref, slot_ref, q_ref, kv0_ref, s1_ref, s3_ref, r1_ref, r2_ref, r3_ref, o_ref, l_ref, e_ref, top_ref, sum_ref
):
    rows = kv0_ref.shape[0]
    sp, slot = sp_ref[0], slot_ref[0]
    per_class, per_residue = rows // CLASSES, rows // WIDE_DILATION
    runs = [pl.ds(c * per_class, per_class) for c in range(CLASSES)]
    jh, ih = run_of_halo(per_residue, 1)
    tail = jnp.concatenate([16 * ih + 4 * jh + c - rows for c in range(CLASSES)], axis=1)
    tk = jnp.concatenate([positions(rows, 1), tail], axis=1)
    bias = bias_of(positions(rows, 0), tk, (tk >= 0) | (sp >= 1), slope_of(0, slot))
    keys = jnp.concatenate([kv0_ref[...], r1_ref[0:STEPS, :]], axis=0)
    p, l0 = softmax_pieces(dot(q_ref[:, 0:HEAD_DIM], keys[:, 0:HEAD_DIM], NT) + bias)
    o0 = dot(p, keys[:, HEAD_DIM:PAIR], NN)
    jq, iq = run_of_class(per_class, 0)
    jk, ik = run_of_class(per_class, 1)
    own = 4 * ik + jk
    tk = jnp.concatenate([own, own - per_class, 4 * ih + jh - 2 * per_class], axis=1)
    block = jnp.concatenate([jnp.zeros_like(own), jnp.full_like(own, 1), jnp.full_like(jh, 2)], axis=1)
    bias = bias_of(4 * iq + jq, tk, block <= sp, slope_of(1, slot))
    halo = STEPS // CLASSES
    keys = [
        jnp.concatenate(
            [
                s1_ref[pl.ds(STEPS + c * per_class, per_class), :],
                r1_ref[pl.ds(STEPS + c * per_class, per_class), :],
                r2_ref[pl.ds(c * halo, halo), :],
            ],
            axis=0,
        )
        for c in range(CLASSES)
    ]
    scores = [dot(q_ref[runs[c], HEAD_DIM : 2 * HEAD_DIM], keys[c][:, 0:HEAD_DIM], NT) + bias for c in range(CLASSES)]
    p, l1 = softmax_pieces(jnp.concatenate(scores, axis=0))
    o1 = [
        dot(p[c * per_class : (c + 1) * per_class], keys[c][:, HEAD_DIM:PAIR], NN) for c in range(CLASSES)
    ]
    top = jnp.maximum(l0, l1)
    w0, w1 = jnp.exp(l0 - top), jnp.exp(l1 - top)
    both = w0 + w1
    l_ref[...] = top + jnp.log(both)
    both = 1.0 / both
    o_ref[...] = (w0 * both) * o0 + (w1 * both) * jnp.concatenate(o1, axis=0)
    bias = wide_bias(rows, (0, 1, 2, 3), sp, slope_of(2, slot))
    scores = []
    for c in range(CLASSES):
        lo = c * per_class
        keys = jnp.concatenate(
            [
                s3_ref[runs[c], 0:HEAD_DIM],
                r1_ref[pl.ds(STEPS + rows + lo, per_class), 0:HEAD_DIM],
                r2_ref[pl.ds(STEPS + lo, per_class), 0:HEAD_DIM],
                r3_ref[runs[c], 0:HEAD_DIM],
            ],
            axis=0,
        )
        scores.append(dot(q_ref[runs[c], 2 * HEAD_DIM : 3 * HEAD_DIM], keys, NT) + bias)
    scores = jnp.concatenate(scores, axis=0)
    top = jnp.max(scores, axis=-1, keepdims=True)
    e = jnp.exp(scores - top)
    e_ref[...] = e
    top_ref[...] = top
    sum_ref[...] = jnp.sum(e, axis=-1, keepdims=True)


def late_kernel(
    sp_ref, slot_ref, q_ref, s3_ref, r1_ref, r2_ref, r3_ref, r4_ref, o_ref, l_ref, e_ref, top_ref, sum_ref, mix_ref, lw_ref
):
    rows = s3_ref.shape[0]
    sp, slot = sp_ref[0], slot_ref[0]
    per_class = rows // CLASSES
    halo = STEPS // CLASSES
    runs = [pl.ds(c * per_class, per_class) for c in range(CLASSES)]
    bias = wide_bias(rows, (4, 5), sp, slope_of(2, slot), halo_block=6)
    keys = [
        jnp.concatenate(
            [r4_ref[runs[c], :], r4_ref[pl.ds(rows + c * per_class, per_class), :], r4_ref[pl.ds(2 * rows + c * halo, halo), :]],
            axis=0,
        )
        for c in range(CLASSES)
    ]
    scores = jnp.concatenate(
        [dot(q_ref[runs[c], 2 * HEAD_DIM : 3 * HEAD_DIM], keys[c][:, 0:HEAD_DIM], NT) + bias for c in range(CLASSES)], axis=0
    )
    top0 = top_ref[...]
    top = jnp.maximum(top0, jnp.max(scores, axis=-1, keepdims=True))
    e = jnp.exp(scores - top)
    shrink = jnp.exp(top0 - top)
    total = sum_ref[...] * shrink + jnp.sum(e, axis=-1, keepdims=True)
    scale = 1.0 / total
    l2 = top + jnp.log(total)
    p = (e * scale).astype(jnp.bfloat16)
    p_early = (e_ref[...] * (shrink * scale)).astype(jnp.bfloat16)
    out = []
    for c in range(CLASSES):
        lo = c * per_class
        early = jnp.concatenate(
            [
                s3_ref[runs[c], HEAD_DIM:PAIR],
                r1_ref[pl.ds(STEPS + rows + lo, per_class), HEAD_DIM:PAIR],
                r2_ref[pl.ds(STEPS + lo, per_class), HEAD_DIM:PAIR],
                r3_ref[runs[c], HEAD_DIM:PAIR],
            ],
            axis=0,
        )
        out.append(
            dot(p_early[lo : lo + per_class], early, NN) + dot(p[lo : lo + per_class], keys[c][:, HEAD_DIM:PAIR], NN)
        )
    l01 = l_ref[...]
    top = jnp.maximum(l01, l2)
    w01, w2 = jnp.exp(l01 - top), jnp.exp(l2 - top)
    both = w01 + w2
    lw_ref[...] = top + jnp.log(both)
    both = 1.0 / both
    mixed = ((w01 * both) * o_ref[...] + (w2 * both) * jnp.concatenate(out, axis=0)).astype(jnp.bfloat16)
    mix = dot(mixed, to_class_order(rows).astype(jnp.bfloat16), TN).astype(jnp.bfloat16)
    for n in range(mix_ref.shape[0]):
        mix_ref[n] = mix


def output_kernel(mix_ref, w_ref, lw_ref, out_ref, log_weight_ref):
    rows = out_ref.shape[0]
    log_weight_ref[...] = jnp.sum(jnp.where(to_class_order(rows), lw_ref[...], 0.0), axis=0, keepdims=True)
    out_ref[...] = dot(mix_ref[...].reshape(-1, rows), w_ref[...], TN).astype(jnp.bfloat16)


VMEM = pl.BlockSpec(memory_space=pltpu.VMEM)
SMEM = pl.BlockSpec(memory_space=pltpu.SMEM)
HBM = pl.BlockSpec(memory_space=pltpu.HBM)


def call(body, operands, outs, specs=None, scratch=()):
    return pl.pallas_call(
        body,
        in_specs=specs or [VMEM] * len(operands),
        out_specs=[VMEM] * len(outs),
        out_shape=[jax.ShapeDtypeStruct(s, d) for s, d in outs],
        scratch_shapes=list(scratch),
        compiler_params=pltpu.CompilerParams(vmem_limit_bytes=20 * 2**20),
    )(*operands)


def in_hbm(value):
    return pltpu.with_memory_space_constraint(value, pltpu.HBM)


def from_behind(value, by):
    devices = lax.axis_size("sp")
    return lax.ppermute(value, "sp", [(i, i + by) for i in range(devices - by)])


def layer(tokens, norm_gain, w_query, w_key, w_value, w_out):
    rows, width = tokens.shape
    bf16, f32 = jnp.bfloat16, jnp.float32
    sp = lax.axis_index("sp").reshape(1)
    slot = lax.axis_index("tp").reshape(1)
    kv0, s1, s2, s3, normed = call(
        project_kernel,
        (in_hbm(tokens), in_hbm(norm_gain.reshape(1, -1)), in_hbm(w_key), in_hbm(w_value)),
        [
            ((rows, PAIR), bf16),
            ((STEPS + 2 * rows, PAIR), bf16),
            ((STEPS + rows, PAIR), bf16),
            ((rows, PAIR), bf16),
            ((rows, width), bf16),
        ],
        specs=[HBM] * 4,
        scratch=[
            pltpu.VMEM((rows, width), bf16),
            pltpu.VMEM((1, width), f32),
            pltpu.VMEM((GROUPS * PAIR, width), bf16),
            pltpu.SemaphoreType.DMA((rows // CHUNK + 2 * GROUPS + 1,)),
        ],
    )
    r1 = from_behind(s1, 1)
    r2 = from_behind(s2, 2)
    r3 = from_behind(s3, 3)
    (q,) = call(query_kernel, (normed, w_query), [((rows, GROUPS * HEAD_DIM), bf16)])
    (s4,) = call(relay_kernel, (s3, r1, r2), [((STEPS + 2 * rows, PAIR), bf16)])
    r4 = from_behind(s4, 4)
    o, l, e, top, total = call(
        early_kernel,
        (sp, slot, q, kv0, s1, s3, r1, r2, r3),
        [((rows, HEAD_DIM), f32), ((rows, 1), f32), ((rows, rows), f32), ((rows, 1), f32), ((rows, 1), f32)],
        specs=[SMEM] * 2 + [VMEM] * 7,
    )
    devices = lax.axis_size("tp")
    mix, lw = call(
        late_kernel,
        (sp, slot, q, s3, r1, r2, r3, r4, o, l, e, top, total),
        [((devices, HEAD_DIM, rows), bf16), ((rows, 1), f32)],
        specs=[SMEM] * 2 + [VMEM] * 11,
    )
    everyone = lax.all_to_all(mix, "tp", 0, 0, tiled=True)
    projected, log_weight = call(
        output_kernel, (everyone, w_out, lw), [((rows, w_out.shape[1]), bf16), ((1, rows), f32)]
    )
    return projected, log_weight


def solution(mesh):
    in_specs = (P("sp", None), P(), P(None, "tp", None), P(None, "tp", None), P(None, "tp", None), P(None, "tp"))
    out_specs = (P("sp", "tp"), P("tp", "sp"))
    return jax.shard_map(layer, mesh=mesh, in_specs=in_specs, out_specs=out_specs, check_vma=False)
```
